32 devices in a mesh: fs: 4 (over z), rep: 4 (over y, x), tp: 2 (over core).
Axes of the slice: x: 2, y: 2, z: 4, core: 2. Of those that a mesh axis runs over, the one named last changes fastest.
Arguments:
- normed_input: bfloat16 [2048, 1024], P(('fs', 'rep')), may hold values from -6 to 6
- query_cotangent: bfloat16 [2048, 512], P(('fs', 'rep'), 'tp'), may hold values from -0.029907227 to 0.029907227
- value_cotangent: bfloat16 [2048, 1024], P(('fs', 'rep'), 'tp'), may hold values from -0.029907227 to 0.029907227
- query_basis: bfloat16 [1024, 128], replicated, may hold values from -0.1875 to 0.1875
- value_basis: bfloat16 [1024, 128], replicated, may hold values from -0.1875 to 0.1875
- query_weight: float32 [1024, 512], P(('fs', 'rep'), 'tp'), may hold values from -0.1875 to 0.1875
- value_weight: float32 [1024, 1024], P(('fs', 'rep'), 'tp'), may hold values from -0.1875 to 0.1875
- query_first: float32 [128, 512], P(('fs', 'rep'), 'tp'), may hold values from -6 to 6
- query_second: float32 [128, 512], P(('fs', 'rep'), 'tp'), may hold values from 0.25 to 4
- value_first: float32 [128, 1024], P(('fs', 'rep'), 'tp'), may hold values from -6 to 6
- value_second: float32 [128, 1024], P(('fs', 'rep'), 'tp'), may hold values from 0.25 to 4
Outputs:
- query_update: float32 [1024, 512], P(('fs', 'rep'), 'tp')
- value_update: float32 [1024, 1024], P(('fs', 'rep'), 'tp')
- query_weight_new: float32 [1024, 512], P(('fs', 'rep'), 'tp')
- value_weight_new: float32 [1024, 1024], P(('fs', 'rep'), 'tp')
- query_first_new: float32 [128, 512], P(('fs', 'rep'), 'tp')
- query_second_new: float32 [128, 512], P(('fs', 'rep'), 'tp')
- value_first_new: float32 [128, 1024], P(('fs', 'rep'), 'tp')
- value_second_new: float32 [128, 1024], P(('fs', 'rep'), 'tp')
- query_copy: bfloat16 [1024, 512], P(None, 'tp')
- value_copy: bfloat16 [1024, 1024], P(None, 'tp')
The draws below stay inside these ranges and needn't reach their ends.
All inputs are finite; a program needn't handle non-finite values.
Results may differ from the reference program's by a relative error of at most 0.001.
Values may be sent and summed in bfloat16 or wider, within the bound.
A program may use at most 64 MiB of HBM per device.

```python
import math
import jax
import jax.numpy as jnp
from jax import lax

D = 1024
RANK = 128
QW = 512
VW = 1024
TOKENS = 2048


def block_levels(stream_key, shape, shards, smallest, top_value):
    gain = 1.0
    for dim, parts in shards:
        steps = jax.random.uniform(jax.random.fold_in(jax.random.fold_in(stream_key, 6), dim), (parts,), jnp.float32, smallest / len(shards), top_value / len(shards))
        gain = gain * jnp.repeat(jnp.exp(steps), shape[dim] // parts).reshape((-1,) + (1,) * (len(shape) - 1 - dim))
    return gain


def normal_values(key, extent, width, most, split=(), dtype=jnp.bfloat16):
    values = jax.random.normal(key, extent, jnp.float32) * width
    if len(split) > 0:
        values = block_levels(key, extent, split, -0.22, 0.18) * values
    return jnp.clip(values, min=-most, max=most).astype(dtype)


def setup_inputs(seed: int = 0) -> dict:
    arg_keys = jax.random.split(jax.random.key(seed), 12)
    normed_input = normal_values(arg_keys[0], (TOKENS, D), 1.0, 6.0, ((0, 16),))
    query_cotangent = normal_values(arg_keys[1], (TOKENS, QW), 0.005, 0.029907227, ((0, 16), (1, 2)))
    value_cotangent = normal_values(arg_keys[2], (TOKENS, VW), 0.005, 0.029907227, ((0, 16), (1, 2)))
    query_basis = normal_values(arg_keys[3], (D, RANK), D ** -0.5, 0.1875)
    value_basis = normal_values(arg_keys[4], (D, RANK), D ** -0.5, 0.1875)
    query_weight = normal_values(arg_keys[5], (D, QW), D ** -0.5, 0.1875, ((0, 16), (1, 2)), jnp.float32)
    value_weight = normal_values(arg_keys[6], (D, VW), D ** -0.5, 0.1875, ((0, 16), (1, 2)), jnp.float32)
    query_first = normal_values(arg_keys[7], (RANK, QW), 1.0, 6.0, ((0, 16), (1, 2)), jnp.float32)
    query_second = jnp.clip(jnp.exp(math.log(4.0) - 2.7725887 * jax.random.uniform(arg_keys[8], (RANK, QW), jnp.float32) ** block_levels(arg_keys[8], (RANK, QW), ((0, 16), (1, 2)), -0.2, 0.2)), 0.25, 4.0)
    value_first = normal_values(arg_keys[9], (RANK, VW), 1.0, 6.0, ((0, 16), (1, 2)), jnp.float32)
    value_second = jnp.clip(jnp.exp(math.log(4.0) - 2.7725887 * jax.random.uniform(arg_keys[10], (RANK, VW), jnp.float32) ** block_levels(arg_keys[10], (RANK, VW), ((0, 16), (1, 2)), -0.2, 0.2)), 0.25, 4.0)
    return dict(normed_input=normed_input, query_cotangent=query_cotangent, value_cotangent=value_cotangent, query_basis=query_basis, value_basis=value_basis, query_weight=query_weight, value_weight=value_weight, query_first=query_first, query_second=query_second, value_first=value_first, value_second=value_second)


def update_matrix(normed_input, cotangent, basis, weight, first_old, second_old):
    gradient = jnp.dot(normed_input.T, cotangent, preferred_element_type=jnp.float32)
    basis_wide = basis.astype(jnp.float32)
    projected = jnp.dot(basis_wide.T, gradient, precision=lax.Precision.HIGHEST)
    first_new = 0.9 * first_old + 0.1 * projected
    second_new = 0.99 * second_old + 0.01 * projected * projected
    direction = first_new / (jnp.sqrt(second_new) + 1e-08)
    norm_scale = jnp.sqrt(jnp.mean(direction * direction) + 1.0)
    update = jnp.dot(basis_wide, direction, precision=lax.Precision.HIGHEST) / norm_scale
    weight_new = weight - 0.01 * update
    return (update, weight_new, first_new, second_new, weight_new.astype(jnp.bfloat16))

def reference(normed_input, query_cotangent, value_cotangent, query_basis, value_basis, query_weight, value_weight, query_first, query_second, value_first, value_second):
    query_out = update_matrix(normed_input, query_cotangent, query_basis, query_weight, query_first, query_second)
    value_out = update_matrix(normed_input, value_cotangent, value_basis, value_weight, value_first, value_second)
    return (query_out[0], value_out[0], query_out[1], value_out[1], query_out[2], query_out[3], value_out[2], value_out[3], query_out[4], value_out[4])
```

```python
import functools
import jax
import jax.numpy as jnp
from jax import lax
from jax.experimental import pallas as pl
from jax.experimental.pallas import tpu as pltpu
from jax.sharding import PartitionSpec as P


def moments(projected, first_old, second_old):
    first_new = 0.9 * first_old + 0.1 * projected
    second_new = 0.99 * second_old + 0.01 * projected * projected
    return (first_new, second_new, first_new / (jnp.sqrt(second_new) + 1e-08))


def finish(whole_dir, basis_rows, weight, squares, entries):
    norm_scale = jnp.sqrt(squares / entries + 1.0)
    update = jnp.dot(basis_rows, whole_dir, precision=lax.Precision.HIGHEST) / norm_scale
    weight_new = weight - 0.01 * update
    return (update, weight_new, weight_new.astype(jnp.bfloat16))


def split_parts(reduced):
    high_part = reduced.astype(jnp.bfloat16)
    held = lax.optimization_barrier(high_part)
    low_part = (reduced - held.astype(jnp.float32)).astype(jnp.bfloat16)
    return (high_part, low_part)


def parts_product(high_part, low_part, cotangent):
    dims = (((0,), (0,)), ((), ()))
    first_term = lax.dot_general(high_part, cotangent, dims, preferred_element_type=jnp.float32)
    second_term = lax.dot_general(low_part, cotangent, dims, preferred_element_type=jnp.float32)
    return first_term + second_term


def body(
    normed_input,
    query_cotangent,
    value_cotangent,
    query_basis,
    value_basis,
    query_weight,
    value_weight,
    query_first,
    query_second,
    value_first,
    value_second,
):
    row_count = query_weight.shape[0]
    query_width = query_cotangent.shape[1]
    offset = lax.axis_index(("fs", "rep")) * row_count
    query_rows = lax.dynamic_slice_in_dim(query_basis, offset, row_count, 0).astype(jnp.float32)
    value_rows = lax.dynamic_slice_in_dim(value_basis, offset, row_count, 0).astype(jnp.float32)
    reduced_query = jnp.dot(normed_input, query_basis, preferred_element_type=jnp.float32)
    reduced_value = jnp.dot(normed_input, value_basis, preferred_element_type=jnp.float32)
    query_high, query_low = split_parts(reduced_query)
    value_high, value_low = split_parts(reduced_value)
    projected = lax.psum_scatter(
        jnp.concatenate(
            [
                parts_product(query_high, query_low, query_cotangent),
                parts_product(value_high, value_low, value_cotangent),
            ],
            axis=1,
        ),
        ("fs", "rep"),
        scatter_dimension=0,
        tiled=True,
    )
    query_projected = projected[:, :query_width]
    value_projected = projected[:, query_width:]
    query_first_new, query_second_new, query_dir = moments(
        query_projected, query_first, query_second
    )
    value_first_new, value_second_new, value_dir = moments(
        value_projected, value_first, value_second
    )
    query_whole, value_whole = (
        lax.all_gather(query_dir, ("fs", "rep"), axis=0, tiled=True),
        lax.all_gather(value_dir, ("fs", "rep"), axis=0, tiled=True),
    )
    query_squares, value_squares = lax.psum(
        (jnp.sum(query_dir * query_dir), jnp.sum(value_dir * value_dir)), ("fs", "rep", "tp")
    )
    tp_count = lax.axis_size("tp")
    query_update, query_weight_new, query_half = finish(
        query_whole,
        query_rows,
        query_weight,
        query_squares,
        query_whole.shape[0] * query_whole.shape[1] * tp_count,
    )
    value_update, value_weight_new, value_half = finish(
        value_whole,
        value_rows,
        value_weight,
        value_squares,
        value_whole.shape[0] * value_whole.shape[1] * tp_count,
    )
    query_copy, value_copy = (
        lax.all_gather(query_half, ("fs", "rep"), axis=0, tiled=True),
        lax.all_gather(value_half, ("fs", "rep"), axis=0, tiled=True),
    )
    return (
        query_update,
        value_update,
        query_weight_new,
        value_weight_new,
        query_first_new,
        query_second_new,
        value_first_new,
        value_second_new,
        query_copy,
        value_copy,
    )


MESH = pl.DeviceIdType.MESH
VMEM_LIMIT = 60 * 2**20
OUT_LIMIT = 16 * 2**20
CHUNKS = (0, 1)
EARLY_Z = (1, 2)
OFF_Z = True
PLAN = {
    "sent": (("z", 1, 0), ("z", 1, 1)),
    "second0": (("r", 0, 0), ("r", 1, 0)),
    "second1": (("r", 0, 1), ("r", 1, 1)),
    "third0": (("z", 2, 0),),
    "third1": (("z", 2, 1),),
}
f32, bf16 = jnp.float32, jnp.bfloat16


def scope(name):
    pass


def two_parts(x):
    high = x.astype(bf16)
    return high, (x - high.astype(f32)).astype(bf16)


def size_of(ref):
    n = jnp.dtype(ref.dtype).itemsize
    for d in ref.shape:
        n *= d
    return n


def kernel(
    T,
    x_hbm, qc_hbm, vc_hbm, qb_hbm, vb_hbm, qw_hbm, vw_hbm, qf_hbm, qs_hbm, vf_hbm, vs_hbm,
    qu, vu, qn, vn, qfn, vfn, qsn, vsn, qcopy, vcopy,
    x_ref, qc, vc, qb, vb, qw, vw, qf, vf, qs, vs,
    qzw, vzw, qrw, vrw, qpart, vpart, qgot1, vgot1, qmid, vmid, qgot2, vgot2, qdirs, vdirs,
    qsq, vsq, qsq_in, vsq_in, spare,
    load, sent, in1, in2, in3, in4, in5, in6, in7, in8, in9, in10, rest,
):
    F, R = 4, 4
    z, r, t = lax.axis_index("fs"), lax.axis_index("rep"), lax.axis_index("tp")
    zs = [z, z + 1 - 2 * lax.rem(z, 2), 3 - z, lax.rem(z + 2, 4)]
    rs = [r, r + 1 - 2 * lax.rem(r, 2), lax.rem(r + 2, 4), 3 - r]
    ts = [lax.rem(t + k, T) for k in range(T)]
    rows, M = qw.shape[0], qf.shape[0]
    cot, basis, weight, first, second = (qc, vc), (qb, vb), (qw, vw), (qf, vf), (qs, vs)
    update_out, weight_out, first_out, second_out = (qu, vu), (qn, vn), (qfn, vfn), (qsn, vsn)
    copy, z_weight, r_weight = (qcopy, vcopy), (qzw, vzw), (qrw, vrw)
    part, got1, mid, got2, dirs = (qpart, vpart), (qgot1, vgot1), (qmid, vmid), (qgot2, vgot2), (qdirs, vdirs)
    squares, squares_in = (qsq, vsq), (qsq_in, vsq_in)
    width = [w.shape[1] for w in weight]

    total_sent, total_rest = [], []

    def remote(src, dst, received, peer, last=False):
        d = pltpu.make_async_remote_copy(
            src_ref=src,
            dst_ref=dst,
            send_sem=sent.at[0],
            recv_sem=received,
            device_id=peer,
            device_id_type=MESH,
        )
        d.start()
        total_sent.append(size_of(src))
        if last:
            total_rest.append(size_of(src))
        return d

    def settle(ref, sem):
        pltpu.make_async_copy(ref, ref, sem).wait()

    scope("p00_sig_load")
    barrier = pltpu.get_barrier_semaphore()
    for axis, others in (("rep", rs), ("fs", zs), ("tp", ts)):
        for other in others[1:]:
            pl.semaphore_signal(barrier, inc=1, device_id={axis: other}, device_id_type=MESH)
    sources = {
        "x": (x_hbm, x_ref),
        ("basis", 0): (qb_hbm, qb), ("cot", 0): (qc_hbm, qc),
        ("basis", 1): (vb_hbm, vb), ("cot", 1): (vc_hbm, vc),
        ("weight", 0): (qw_hbm, qw), ("weight", 1): (vw_hbm, vw),
        ("first", 0): (qf_hbm, qf), ("first", 1): (vf_hbm, vf),
        ("second", 0): (qs_hbm, qs), ("second", 1): (vs_hbm, vs),
    }
    names = ["x"] + [(n, c) for c in CHUNKS for n in ("basis", "cot")]
    names += [(n, c) for n in ("weight", "first", "second") for c in CHUNKS]
    loads = {
        n: pltpu.make_async_copy(sources[n][0], sources[n][1], load.at[i])
        for i, n in enumerate(names)
    }
    for c in loads.values():
        c.start()

    early = {}

    def run(point):
        for kind, k, c in PLAN.get(point, ()):
            if ("weight", c) in loads:
                loads.pop(("weight", c)).wait()
            if kind == "z":
                d = remote(weight[c], z_weight[c].at[k - 1], in8.at[c, k - 1], {"fs": zs[k]})
            else:
                d = remote(weight[c], r_weight[c].at[k], in9.at[c, k], {"rep": rs[k + 1]})
            early[kind, k, c] = d

    far = (2, 3, 1, 0)
    for i, c in enumerate(CHUNKS):
        scope(f"p01_load_dot#c={c}")
        if i == 0:
            loads.pop("x").wait()
            x = x_ref[...]
        loads.pop(("basis", c)).wait()
        reduced = jnp.dot(x, basis[c][...], preferred_element_type=f32).T
        high, low = two_parts(reduced)
        both = jnp.concatenate([high, low], axis=1)
        loads.pop(("cot", c)).wait()
        g = cot[c][...]
        total = jnp.dot(both, jnp.concatenate([g, g], axis=0), preferred_element_type=f32)
        for a in range(F):
            for b in range(R):
                at = (a * R + b) * M
                part[c][b, a] = total[at : at + M]
        if i == 0:
            scope("p02_barrier")
            pl.semaphore_wait(barrier, F + R + T - 3)
        scope(f"p03_send1#c={c}")
        for j in far:
            for k in range(1, R):
                remote(part[c].at[rs[k], zs[j]], got1[c].at[k, j], in1.at[c, j], {"rep": rs[k]})
    run("sent")

    own = {}
    for c in CHUNKS:
        scope(f"p04_recv1#c={c}")
        for j in far:
            total = part[c][r, zs[j]]
            settle(got1[c].at[1:R, j], in1.at[c, j])
            for k in range(1, R):
                total = total + got1[c][k, j]
            if j > 0:
                mid[c][j] = total
                remote(mid[c].at[j], got2[c].at[j], in2.at[c], {"fs": zs[j]})
            else:
                own[c] = total
        run(f"second{c}")

    third = {}

    def spread(c, j):
        block = dirs[c].at[zs[j], r]
        for k in range(1, R):
            remote(block, block, in4.at[c], {"rep": rs[k]})

    for c in CHUNKS:
        scope(f"p05_recv2#c={c}")
        loads.pop(("first", c)).wait()
        loads.pop(("second", c)).wait()
        projected = own[c]
        settle(got2[c].at[1:F], in2.at[c])
        for j in (1, 3, 2):
            projected = projected + got2[c][j]
        fn = 0.9 * first[c][...] + 0.1 * projected
        sn = 0.99 * second[c][...] + 0.01 * projected * projected
        dirs[c][z, r] = fn / (jnp.sqrt(sn) + 1e-08)
        block = dirs[c].at[z, r]
        for j in (2, 3, 1):
            third[c, j] = remote(block, block, in3.at[c, j - 1], {"fs": zs[j]})
        spread(c, 0)
        first_out[c][...] = fn
        second_out[c][...] = sn
        run(f"third{c}")

    for c in CHUNKS:
        scope(f"p06_recv3#c={c}")
        for j in (1, 3, 2):
            third[c, j].wait_recv()
            spread(c, j)
        run(f"fourth{c}")

    def start_of(j, k):
        return pl.multiple_of((zs[j] * R + rs[k]) * rows, rows)

    size = rows // 2

    def piece(c, j, k, p):
        at = pl.multiple_of(start_of(j, k) + p * size, size)
        return copy[c].at[pl.ds(at, size), :]

    def product(c, dd, blocks):
        b = jnp.concatenate([basis[c][pl.ds(start_of(j, k), rows), :] for j, k in blocks], axis=0)
        return jnp.dot(jnp.concatenate([b, b], axis=1), dd, preferred_element_type=f32)

    direct, across, sixth = {}, {}, {}

    def pass_on(c, j, a):
        block = piece(c, j, a + 1, a)
        remote(block, block, rest.at[0], {"rep": rs[2 - a]}, True)

    def send_direct(c, j, order=((0, 0), (1, 1), (0, 1), (1, 0))):
        for a, p in order:
            block = piece(c, j, 0, p)
            if a == p:
                direct[c, j, a] = remote(block, block, in7.at[c, j - 1, a], {"rep": rs[a + 1]})
            else:
                remote(block, block, rest.at[0], {"rep": rs[a + 1]}, True)

    late = [j for j in range(1, F) if j not in EARLY_Z]
    for c in CHUNKS:
        scope(f"p07_recv4#c={c}")
        settle(dirs[c].at[:, 1:R], in4.at[c])
        scope(f"p08_square#c={c}")
        whole = dirs[c][...].reshape(F * R * M, width[c])
        d = (whole * whole).reshape(F * R * M // 8, 8, width[c]).sum(axis=0)
        acc = d[:, :128]
        for b in range(1, width[c] // 128):
            acc = acc + d[:, b * 128 : (b + 1) * 128]
        squares[c][...] = acc
        for k in range(1, T):
            remote(squares[c], squares_in[c].at[k], in5.at[c], {"tp": ts[k]})
        dd = jnp.concatenate(two_parts(whole), axis=0)
        lines = [(0, 0)] + [(k, 0) for k in EARLY_Z]
        raw = product(c, dd, lines)
        sides = [(0, 1), (0, 2)]
        raw_side = product(c, dd, sides)
        scope(f"p09_fifth#c={c}")
        settle(squares_in[c].at[1:T], in5.at[c])
        sq = squares[c][...]
        for k in range(1, T):
            sq = sq + squares_in[c][k]
        scale = jnp.sqrt(jnp.sum(sq, keepdims=True) / (F * R * M * width[c] * T) + 1.0)
        inverse = 1.0 / scale
        if ("weight", c) in loads:
            loads.pop(("weight", c)).wait()
        scope(f"p10_copy#c={c}")
        for n, (j, k) in enumerate(lines):
            update = raw[n * rows : (n + 1) * rows] * inverse
            if n == 0:
                new = weight[c][...] - 0.01 * update
                update_out[c][...] = update
                weight_out[c][...] = new
            else:
                early["z", j, c].wait_recv()
                new = z_weight[c][j - 1] - 0.01 * update
            copy[c][pl.ds(start_of(j, k), rows), :] = new.astype(bf16)
            if n == 0:
                for j2 in late:
                    block = copy[c].at[pl.ds(start_of(0, 0), rows), :]
                    sixth[c, j2] = remote(block, block, in6.at[c, j2 - 1], {"fs": zs[j2]})
            elif not (OFF_Z and j == 1):
                send_direct(c, j)
        scope(f"p11_side#c={c}")
        for n, (j, k) in enumerate(sides):
            update = raw_side[n * rows : (n + 1) * rows] * inverse
            early["r", n, c].wait_recv()
            new = r_weight[c][n] - 0.01 * update
            copy[c][pl.ds(start_of(j, k), rows), :] = new.astype(bf16)
            if OFF_Z:
                block = piece(c, 0, k, n)
                across[c, n] = remote(block, block, in10.at[c, n], {"fs": zs[1]})
                block = piece(c, 0, k, 1 - n)
                remote(block, block, rest.at[0], {"fs": zs[1]}, True)
        for a in range(2):
            pass_on(c, 0, a)
        run(f"final{c}")

    for c in CHUNKS:
        scope(f"p12_sixth#c={c}")
        for j in late:
            sixth[c, j].wait_recv()
            send_direct(c, j)
    for c in CHUNKS:
        for j in range(1, F):
            if j in late:
                continue
            scope(f"p13_pass#c={c}#j={j}")
            for a in range(2):
                (across[c, a] if OFF_Z and j == 1 else direct[c, j, a]).wait_recv()
                pass_on(c, j, a)
    for c in CHUNKS:
        for j in late:
            scope(f"p14_pass#c={c}#j={j}")
            for a in range(2):
                direct[c, j, a].wait_recv()
                pass_on(c, j, a)
    scope("p15_last")
    settle(spare.at[: sum(total_rest) // 512], rest.at[0])
    scope("p16_waitsend")
    settle(spare.at[: sum(total_sent) // 512], sent.at[0])
    scope(None)


def write_out(*refs):
    sem, sources, targets = refs[20], refs[:10], refs[10:20]
    copies = [
        pltpu.make_async_copy(src, dst, sem.at[i])
        for i, (src, dst) in enumerate(zip(sources, targets))
    ]
    for c in copies[::-1]:
        c.start()
    for c in copies[::-1]:
        c.wait()


def fused(plain, *args):
    x, qc, vc, qb, vb, qw, vw, qf, qs, vf, vs = args
    F, R, T = (lax.axis_size(name) for name in ("fs", "rep", "tp"))
    QC, VC = qc.shape[1], vc.shape[1]
    M, rows = qf.shape[0], qw.shape[0]
    aligned = M % 8 == 0 and rows % 32 == 0 and QC % 128 == 0 and VC % 128 == 0
    if not aligned or F != 4 or R != 4:
        return plain(*args)
    out = jax.ShapeDtypeStruct
    vmem = pl.BlockSpec(memory_space=pltpu.VMEM)
    dma = pltpu.SemaphoreType.DMA
    W = (QC, VC)

    def each(*shape, dtype=f32):
        return [pltpu.VMEM(shape + (w,), dtype) for w in W]

    sems = [
        (11,), (1,), (2, F), (2,), (2, F - 1), (2,), (2,), (2, F - 1), (2, F - 1, 2), (2, F - 1), (2, 2), (2, 2), (1,),
    ]
    results = pl.pallas_call(
        functools.partial(kernel, T),
        out_shape=each(rows) + each(rows) + each(M) + each(M) + each(rows * F * R, dtype=bf16),
        in_specs=[pl.BlockSpec(memory_space=pltpu.HBM)] * 11,
        out_specs=[vmem] * 10,
        scratch_shapes=[
            pltpu.VMEM(x.shape, bf16),
            pltpu.VMEM(qc.shape, bf16),
            pltpu.VMEM(vc.shape, bf16),
            pltpu.VMEM(qb.shape, bf16),
            pltpu.VMEM(vb.shape, bf16),
            *each(rows), *each(M), *each(M),
            *each(F - 1, rows), *each(2, rows),
            *each(R, F, M), *each(R, F, M), *each(F, M), *each(F, M), *each(F, R, M),
            pltpu.VMEM((8, 128), f32), pltpu.VMEM((8, 128), f32),
            pltpu.VMEM((T, 8, 128), f32), pltpu.VMEM((T, 8, 128), f32),
            pltpu.VMEM((8 * rows * F * R, 128), f32),
            *[dma(shape) for shape in sems],
        ],
        compiler_params=pltpu.CompilerParams(
            collective_id=0, has_side_effects=True, vmem_limit_bytes=VMEM_LIMIT
        ),
    )(*args)
    outs = pl.pallas_call(
        write_out,
        out_shape=[
            out(qw.shape, f32), out(vw.shape, f32), out(qw.shape, f32), out(vw.shape, f32),
            out(qf.shape, f32), out(vf.shape, f32), out(qf.shape, f32), out(vf.shape, f32),
            out((rows * F * R, QC), bf16), out((rows * F * R, VC), bf16),
        ],
        in_specs=[vmem] * 10,
        out_specs=[pl.BlockSpec(memory_space=pltpu.HBM)] * 10,
        scratch_shapes=[dma((10,))],
        compiler_params=pltpu.CompilerParams(vmem_limit_bytes=OUT_LIMIT),
    )(*results)
    qu, vu, qn, vn, qfn, vfn, qsn, vsn, qcopy, vcopy = outs
    return (qu, vu, qn, vn, qfn, qsn, vfn, vsn, qcopy, vcopy)


def solution(mesh):
    in_specs = (
        P(("fs", "rep"), None),
        P(("fs", "rep"), "tp"),
        P(("fs", "rep"), "tp"),
        P(),
        P(),
        P(("fs", "rep"), "tp"),
        P(("fs", "rep"), "tp"),
        P(("fs", "rep"), "tp"),
        P(("fs", "rep"), "tp"),
        P(("fs", "rep"), "tp"),
        P(("fs", "rep"), "tp"),
    )
    out_specs = (
        P(("fs", "rep"), "tp"),
        P(("fs", "rep"), "tp"),
        P(("fs", "rep"), "tp"),
        P(("fs", "rep"), "tp"),
        P(("fs", "rep"), "tp"),
        P(("fs", "rep"), "tp"),
        P(("fs", "rep"), "tp"),
        P(("fs", "rep"), "tp"),
        P(None, "tp"),
        P(None, "tp"),
    )
    return jax.shard_map(functools.partial(fused, body), mesh=mesh, in_specs=in_specs, out_specs=out_specs, check_vma=False)
```

```python
import functools
import jax
import jax.numpy as jnp
from jax import lax
from jax.experimental import pallas as pl
from jax.experimental.pallas import tpu as pltpu
from jax.sharding import PartitionSpec as P


def moments(projected, first_old, second_old):
    first_new = 0.9 * first_old + 0.1 * projected
    second_new = 0.99 * second_old + 0.01 * projected * projected
    return (first_new, second_new, first_new / (jnp.sqrt(second_new) + 1e-08))


def finish(whole_dir, basis_rows, weight, squares, entries):
    norm_scale = jnp.sqrt(squares / entries + 1.0)
    update = jnp.dot(basis_rows, whole_dir, precision=lax.Precision.HIGHEST) / norm_scale
    weight_new = weight - 0.01 * update
    return (update, weight_new, weight_new.astype(jnp.bfloat16))


def split_parts(reduced):
    high_part = reduced.astype(jnp.bfloat16)
    held = lax.optimization_barrier(high_part)
    low_part = (reduced - held.astype(jnp.float32)).astype(jnp.bfloat16)
    return (high_part, low_part)


def parts_product(high_part, low_part, cotangent):
    dims = (((0,), (0,)), ((), ()))
    first_term = lax.dot_general(high_part, cotangent, dims, preferred_element_type=jnp.float32)
    second_term = lax.dot_general(low_part, cotangent, dims, preferred_element_type=jnp.float32)
    return first_term + second_term


def body(
    normed_input,
    query_cotangent,
    value_cotangent,
    query_basis,
    value_basis,
    query_weight,
    value_weight,
    query_first,
    query_second,
    value_first,
    value_second,
):
    row_count = query_weight.shape[0]
    query_width = query_cotangent.shape[1]
    offset = lax.axis_index(("fs", "rep")) * row_count
    query_rows = lax.dynamic_slice_in_dim(query_basis, offset, row_count, 0).astype(jnp.float32)
    value_rows = lax.dynamic_slice_in_dim(value_basis, offset, row_count, 0).astype(jnp.float32)
    reduced_query = jnp.dot(normed_input, query_basis, preferred_element_type=jnp.float32)
    reduced_value = jnp.dot(normed_input, value_basis, preferred_element_type=jnp.float32)
    query_high, query_low = split_parts(reduced_query)
    value_high, value_low = split_parts(reduced_value)
    projected = lax.psum_scatter(
        jnp.concatenate(
            [
                parts_product(query_high, query_low, query_cotangent),
                parts_product(value_high, value_low, value_cotangent),
            ],
            axis=1,
        ),
        ("fs", "rep"),
        scatter_dimension=0,
        tiled=True,
    )
    query_projected = projected[:, :query_width]
    value_projected = projected[:, query_width:]
    query_first_new, query_second_new, query_dir = moments(
        query_projected, query_first, query_second
    )
    value_first_new, value_second_new, value_dir = moments(
        value_projected, value_first, value_second
    )
    query_whole, value_whole = (
        lax.all_gather(query_dir, ("fs", "rep"), axis=0, tiled=True),
        lax.all_gather(value_dir, ("fs", "rep"), axis=0, tiled=True),
    )
    query_squares, value_squares = lax.psum(
        (jnp.sum(query_dir * query_dir), jnp.sum(value_dir * value_dir)), ("fs", "rep", "tp")
    )
    tp_count = lax.axis_size("tp")
    query_update, query_weight_new, query_half = finish(
        query_whole,
        query_rows,
        query_weight,
        query_squares,
        query_whole.shape[0] * query_whole.shape[1] * tp_count,
    )
    value_update, value_weight_new, value_half = finish(
        value_whole,
        value_rows,
        value_weight,
        value_squares,
        value_whole.shape[0] * value_whole.shape[1] * tp_count,
    )
    query_copy, value_copy = (
        lax.all_gather(query_half, ("fs", "rep"), axis=0, tiled=True),
        lax.all_gather(value_half, ("fs", "rep"), axis=0, tiled=True),
    )
    return (
        query_update,
        value_update,
        query_weight_new,
        value_weight_new,
        query_first_new,
        query_second_new,
        value_first_new,
        value_second_new,
        query_copy,
        value_copy,
    )


MESH = pl.DeviceIdType.MESH
VMEM_LIMIT = 60 * 2**20
OUT_LIMIT = 16 * 2**20
CHUNKS = (0, 1)
EARLY_Z = (1, 2)
OFF_Z = True
PLAN = {'sent': (('z', 2, 0), ('z', 1, 1)), 'second0': (('r', 0, 0), ('r', 1, 0)), 'second1': (('r', 0, 1), ('r', 1, 1)), 'fourth1': (('z', 1, 0), ('z', 2, 1))}
f32, bf16 = jnp.float32, jnp.bfloat16


def scope(name):
    pass


def two_parts(x):
    high = x.astype(bf16)
    return high, (x - high.astype(f32)).astype(bf16)


def size_of(ref):
    n = jnp.dtype(ref.dtype).itemsize
    for d in ref.shape:
        n *= d
    return n


def kernel(
    T,
    x_hbm, qc_hbm, vc_hbm, qb_hbm, vb_hbm, qw_hbm, vw_hbm, qf_hbm, qs_hbm, vf_hbm, vs_hbm,
    qu, vu, qn, vn, qfn, vfn, qsn, vsn, qcopy, vcopy,
    x_ref, qc, vc, qb, vb, qw, vw, qf, vf, qs, vs,
    qzw, vzw, qrw, vrw, qpart, vpart, qgot1, vgot1, qmid, vmid, qgot2, vgot2, qdirs, vdirs,
    norms, spare,
    load, sent, in1, in2, in3, in4, in5, in6, in7, in8, in9, in10, rest,
):
    F, R = 4, 4
    z, r, t = lax.axis_index("fs"), lax.axis_index("rep"), lax.axis_index("tp")
    zs = [z, z + 1 - 2 * lax.rem(z, 2), 3 - z, lax.rem(z + 2, 4)]
    rs = [r, r + 1 - 2 * lax.rem(r, 2), lax.rem(r + 2, 4), 3 - r]
    ts = [lax.rem(t + k, T) for k in range(T)]
    rows, M = qw.shape[0], qf.shape[0]
    cot, basis, weight, first, second = (qc, vc), (qb, vb), (qw, vw), (qf, vf), (qs, vs)
    update_out, weight_out, first_out, second_out = (qu, vu), (qn, vn), (qfn, vfn), (qsn, vsn)
    copy, z_weight, r_weight = (qcopy, vcopy), (qzw, vzw), (qrw, vrw)
    part, got1, mid, got2, dirs = (qpart, vpart), (qgot1, vgot1), (qmid, vmid), (qgot2, vgot2), (qdirs, vdirs)
    width = [w.shape[1] for w in weight]

    total_sent, total_rest = [], []

    def remote(src, dst, received, peer, last=False):
        d = pltpu.make_async_remote_copy(
            src_ref=src,
            dst_ref=dst,
            send_sem=sent.at[0],
            recv_sem=received,
            device_id=peer,
            device_id_type=MESH,
        )
        d.start()
        total_sent.append(size_of(src))
        if last:
            total_rest.append(size_of(src))
        return d

    def settle(ref, sem):
        pltpu.make_async_copy(ref, ref, sem).wait()

    scope("p00_sig_load")
    barrier = pltpu.get_barrier_semaphore()
    for axis, others in (("rep", rs), ("fs", zs), ("tp", ts)):
        for other in others[1:]:
            pl.semaphore_signal(barrier, inc=1, device_id={axis: other}, device_id_type=MESH)
    sources = {
        "x": (x_hbm, x_ref),
        ("basis", 0): (qb_hbm, qb), ("cot", 0): (qc_hbm, qc),
        ("basis", 1): (vb_hbm, vb), ("cot", 1): (vc_hbm, vc),
        ("weight", 0): (qw_hbm, qw), ("weight", 1): (vw_hbm, vw),
        ("first", 0): (qf_hbm, qf), ("first", 1): (vf_hbm, vf),
        ("second", 0): (qs_hbm, qs), ("second", 1): (vs_hbm, vs),
    }
    names = ["x"] + [(n, c) for c in CHUNKS for n in ("basis", "cot")]
    names += [(n, c) for n in ("weight", "first", "second") for c in CHUNKS]
    loads = {
        n: pltpu.make_async_copy(sources[n][0], sources[n][1], load.at[i])
        for i, n in enumerate(names)
    }
    for c in loads.values():
        c.start()

    early = {}

    def run(point):
        for kind, k, c in PLAN.get(point, ()):
            if ("weight", c) in loads:
                loads.pop(("weight", c)).wait()
            if kind == "z":
                d = remote(weight[c], z_weight[c].at[k - 1], in8.at[c, k - 1], {"fs": zs[k]})
            else:
                d = remote(weight[c], r_weight[c].at[k], in9.at[c, k], {"rep": rs[k + 1]})
            early[kind, k, c] = d

    far = (2, 3, 1, 0)
    for i, c in enumerate(CHUNKS):
        scope(f"p01_load_dot#c={c}")
        if i == 0:
            loads.pop("x").wait()
            x = x_ref[...]
        loads.pop(("basis", c)).wait()
        reduced = jnp.dot(x, basis[c][...], preferred_element_type=f32).T
        high, low = two_parts(reduced)
        both = jnp.concatenate([high, low], axis=1)
        loads.pop(("cot", c)).wait()
        g = cot[c][...]
        total = jnp.dot(both, jnp.concatenate([g, g], axis=0), preferred_element_type=f32)
        for a in range(F):
            for b in range(R):
                at = (a * R + b) * M
                part[c][b, a] = total[at : at + M]
        if i == 0:
            scope("p02_barrier")
            pl.semaphore_wait(barrier, F + R + T - 3)
        scope(f"p03_send1#c={c}")
        for j in far:
            for k in range(1, R):
                remote(part[c].at[rs[k], zs[j]], got1[c].at[k, j], in1.at[c, j], {"rep": rs[k]})
    run("sent")

    own = {}
    for c in CHUNKS:
        scope(f"p04_recv1#c={c}")
        for j in far:
            total = part[c][r, zs[j]]
            settle(got1[c].at[1:R, j], in1.at[c, j])
            for k in range(1, R):
                total = total + got1[c][k, j]
            if j > 0:
                mid[c][j] = total
                remote(mid[c].at[j], got2[c].at[j], in2.at[c], {"fs": zs[j]})
            else:
                own[c] = total
        run(f"second{c}")

    third, sums = {}, []

    def spread(c, j):
        block = dirs[c].at[zs[j], r]
        for k in range(1, R):
            remote(block, block, in4.at[c], {"rep": rs[k]})

    for c in CHUNKS:
        scope(f"p05_recv2#c={c}")
        loads.pop(("first", c)).wait()
        loads.pop(("second", c)).wait()
        projected = own[c]
        settle(got2[c].at[1:F], in2.at[c])
        for j in (1, 3, 2):
            projected = projected + got2[c][j]
        fn = 0.9 * first[c][...] + 0.1 * projected
        sn = 0.99 * second[c][...] + 0.01 * projected * projected
        dirs[c][z, r] = fn / (jnp.sqrt(sn) + 1e-08)
        sums.append(jnp.sum(dirs[c][z, r] * dirs[c][z, r], keepdims=True))
        if c == CHUNKS[-1]:
            scope("p055_norms")
            lane = lax.broadcasted_iota(jnp.int32, (1, 128), 1)
            slot = (z * R + r) * T + t
            norms[slot] = jnp.where(lane < 64, sums[CHUNKS.index(0)], sums[CHUNKS.index(1)])
            for j in far:
                for k in range(R):
                    for n in range(T):
                        if j or k or n:
                            peer = {"fs": zs[j], "rep": rs[k], "tp": ts[n]}
                            remote(norms.at[slot], norms.at[slot], in5.at[0], peer)
            scope(f"p056_third#c={c}")
        block = dirs[c].at[z, r]
        for j in (2, 3, 1):
            third[c, j] = remote(block, block, in3.at[c, j - 1], {"fs": zs[j]})
        spread(c, 0)
        first_out[c][...] = fn
        second_out[c][...] = sn
        run(f"third{c}")

    for c in CHUNKS:
        scope(f"p06_recv3#c={c}")
        for j in (1, 3, 2):
            third[c, j].wait_recv()
            spread(c, j)
        run(f"fourth{c}")

    def start_of(j, k):
        return pl.multiple_of((zs[j] * R + rs[k]) * rows, rows)

    size = rows // 2

    def piece(c, j, k, p):
        at = pl.multiple_of(start_of(j, k) + p * size, size)
        return copy[c].at[pl.ds(at, size), :]

    def product(c, dd, blocks):
        b = jnp.concatenate([basis[c][pl.ds(start_of(j, k), rows), :] for j, k in blocks], axis=0)
        return jnp.dot(jnp.concatenate([b, b], axis=1), dd, preferred_element_type=f32)

    direct, across, sixth = {}, {}, {}

    def pass_on(c, j, a):
        block = piece(c, j, a + 1, a)
        remote(block, block, rest.at[0], {"rep": rs[2 - a]}, True)

    def send_direct(c, j, order=((0, 0), (1, 1), (0, 1), (1, 0))):
        for a, p in order:
            block = piece(c, j, 0, p)
            if a == p:
                direct[c, j, a] = remote(block, block, in7.at[c, j - 1, a], {"rep": rs[a + 1]})
            else:
                remote(block, block, rest.at[0], {"rep": rs[a + 1]}, True)

    late = [j for j in range(1, F) if j not in EARLY_Z]
    waiting = []
    for c in CHUNKS:
        scope(f"p07_recv4#c={c}")
        settle(dirs[c].at[:, 1:R], in4.at[c])
        scope(f"p08_square#c={c}")
        whole = dirs[c][...].reshape(F * R * M, width[c])
        dd = jnp.concatenate(two_parts(whole), axis=0)
        blocks = [(0, 0), (1, 0), (0, 1), (0, 2)] + [(j, 0) for j in EARLY_Z if j > 1]
        raw = product(c, dd, blocks[:4])
        raw_far = product(c, dd, blocks[4:]) if blocks[4:] else None
        scope(f"p09_fifth#c={c}")
        if c == CHUNKS[0]:
            settle(spare.at[: F * R * T - 1], in5.at[0])
            sq = jnp.sum(norms[...].reshape(F * R * T, 128), axis=0, keepdims=True)
        count = F * R * M * width[c] * T
        inverse = 1.0 / jnp.sqrt(sq[:, 64 * c : 64 * c + 1] / count + 1.0)
        if ("weight", c) in loads:
            loads.pop(("weight", c)).wait()
        scope(f"p10_copy#c={c}")
        for n, (j, k) in enumerate(blocks):
            source = raw if n < 4 else raw_far
            update = source[n % 4 * rows : (n % 4 + 1) * rows] * inverse
            if n == 0:
                new = weight[c][...] - 0.01 * update
                update_out[c][...] = update
                weight_out[c][...] = new
            elif k == 0:
                if j > 1:
                    waiting.append((c, j, update))
                    continue
                early["z", j, c].wait_recv()
                new = z_weight[c][j - 1] - 0.01 * update
            else:
                early["r", k - 1, c].wait_recv()
                new = r_weight[c][k - 1] - 0.01 * update
            copy[c][pl.ds(start_of(j, k), rows), :] = new.astype(bf16)
            if n == 0:
                for j2 in late:
                    block = copy[c].at[pl.ds(start_of(0, 0), rows), :]
                    sixth[c, j2] = remote(block, block, in6.at[c, j2 - 1], {"fs": zs[j2]})
            elif k == 0 and not OFF_Z:
                send_direct(c, j)
            elif k > 0 and OFF_Z:
                block = piece(c, 0, k, k - 1)
                across[c, k - 1] = remote(block, block, in10.at[c, k - 1], {"fs": zs[1]})
                block = piece(c, 0, k, 2 - k)
                remote(block, block, rest.at[0], {"fs": zs[1]}, True)
        for a in range(2):
            pass_on(c, 0, a)
        run(f"final{c}")
    for c, j, update in waiting:
        scope(f"p115_far#c={c}")
        early["z", j, c].wait_recv()
        new = z_weight[c][j - 1] - 0.01 * update
        copy[c][pl.ds(start_of(j, 0), rows), :] = new.astype(bf16)
        send_direct(c, j)

    for c in CHUNKS:
        scope(f"p12_sixth#c={c}")
        for j in late:
            sixth[c, j].wait_recv()
            send_direct(c, j)
    for c in CHUNKS:
        for j in range(1, F):
            if j in late:
                continue
            scope(f"p13_pass#c={c}#j={j}")
            for a in range(2):
                (across[c, a] if OFF_Z and j == 1 else direct[c, j, a]).wait_recv()
                pass_on(c, j, a)
    for c in CHUNKS:
        for j in late:
            scope(f"p14_pass#c={c}#j={j}")
            for a in range(2):
                direct[c, j, a].wait_recv()
                pass_on(c, j, a)
    scope("p15_last")
    settle(spare.at[: sum(total_rest) // 512], rest.at[0])
    scope("p16_waitsend")
    settle(spare.at[: sum(total_sent) // 512], sent.at[0])
    scope(None)


def write_out(*refs):
    sem, sources, targets = refs[20], refs[:10], refs[10:20]
    copies = [
        pltpu.make_async_copy(src, dst, sem.at[i])
        for i, (src, dst) in enumerate(zip(sources, targets))
    ]
    for c in copies[::-1]:
        c.start()
    for c in copies[::-1]:
        c.wait()


def fused(plain, *args):
    x, qc, vc, qb, vb, qw, vw, qf, qs, vf, vs = args
    F, R, T = (lax.axis_size(name) for name in ("fs", "rep", "tp"))
    QC, VC = qc.shape[1], vc.shape[1]
    M, rows = qf.shape[0], qw.shape[0]
    aligned = M % 8 == 0 and rows % 32 == 0 and QC % 128 == 0 and VC % 128 == 0
    if not aligned or F != 4 or R != 4:
        return plain(*args)
    out = jax.ShapeDtypeStruct
    vmem = pl.BlockSpec(memory_space=pltpu.VMEM)
    dma = pltpu.SemaphoreType.DMA
    W = (QC, VC)

    def each(*shape, dtype=f32):
        return [pltpu.VMEM(shape + (w,), dtype) for w in W]

    sems = [
        (11,), (1,), (2, F), (2,), (2, F - 1), (2,), (1,), (2, F - 1), (2, F - 1, 2), (2, F - 1), (2, 2), (2, 2), (1,),
    ]
    results = pl.pallas_call(
        functools.partial(kernel, T),
        out_shape=each(rows) + each(rows) + each(M) + each(M) + each(rows * F * R, dtype=bf16),
        in_specs=[pl.BlockSpec(memory_space=pltpu.HBM)] * 11,
        out_specs=[vmem] * 10,
        scratch_shapes=[
            pltpu.VMEM(x.shape, bf16),
            pltpu.VMEM(qc.shape, bf16),
            pltpu.VMEM(vc.shape, bf16),
            pltpu.VMEM(qb.shape, bf16),
            pltpu.VMEM(vb.shape, bf16),
            *each(rows), *each(M), *each(M),
            *each(F - 1, rows), *each(2, rows),
            *each(R, F, M), *each(R, F, M), *each(F, M), *each(F, M), *each(F, R, M),
            pltpu.VMEM((F * R * T, 1, 128), f32),
            pltpu.VMEM((8 * rows * F * R, 128), f32),
            *[dma(shape) for shape in sems],
        ],
        compiler_params=pltpu.CompilerParams(
            collective_id=0, has_side_effects=True, vmem_limit_bytes=VMEM_LIMIT
        ),
    )(*args)
    outs = pl.pallas_call(
        write_out,
        out_shape=[
            out(qw.shape, f32), out(vw.shape, f32), out(qw.shape, f32), out(vw.shape, f32),
            out(qf.shape, f32), out(vf.shape, f32), out(qf.shape, f32), out(vf.shape, f32),
            out((rows * F * R, QC), bf16), out((rows * F * R, VC), bf16),
        ],
        in_specs=[vmem] * 10,
        out_specs=[pl.BlockSpec(memory_space=pltpu.HBM)] * 10,
        scratch_shapes=[dma((10,))],
        compiler_params=pltpu.CompilerParams(vmem_limit_bytes=OUT_LIMIT),
    )(*results)
    qu, vu, qn, vn, qfn, vfn, qsn, vsn, qcopy, vcopy = outs
    return (qu, vu, qn, vn, qfn, qsn, vfn, vsn, qcopy, vcopy)


def solution(mesh):
    in_specs = (
        P(("fs", "rep"), None),
        P(("fs", "rep"), "tp"),
        P(("fs", "rep"), "tp"),
        P(),
        P(),
        P(("fs", "rep"), "tp"),
        P(("fs", "rep"), "tp"),
        P(("fs", "rep"), "tp"),
        P(("fs", "rep"), "tp"),
        P(("fs", "rep"), "tp"),
        P(("fs", "rep"), "tp"),
    )
    out_specs = (
        P(("fs", "rep"), "tp"),
        P(("fs", "rep"), "tp"),
        P(("fs", "rep"), "tp"),
        P(("fs", "rep"), "tp"),
        P(("fs", "rep"), "tp"),
        P(("fs", "rep"), "tp"),
        P(("fs", "rep"), "tp"),
        P(("fs", "rep"), "tp"),
        P(None, "tp"),
        P(None, "tp"),
    )
    return jax.shard_map(functools.partial(fused, body), mesh=mesh, in_specs=in_specs, out_specs=out_specs, check_vma=False)
```

```python
import functools
import jax
import jax.numpy as jnp
from jax import lax
from jax.experimental import pallas as pl
from jax.experimental.pallas import tpu as pltpu
from jax.sharding import PartitionSpec as P


def moments(projected, first_old, second_old):
    first_new = 0.9 * first_old + 0.1 * projected
    second_new = 0.99 * second_old + 0.01 * projected * projected
    return (first_new, second_new, first_new / (jnp.sqrt(second_new) + 1e-08))


def finish(whole_dir, basis_rows, weight, squares, entries):
    norm_scale = jnp.sqrt(squares / entries + 1.0)
    update = jnp.dot(basis_rows, whole_dir, precision=lax.Precision.HIGHEST) / norm_scale
    weight_new = weight - 0.01 * update
    return (update, weight_new, weight_new.astype(jnp.bfloat16))


def split_parts(reduced):
    high_part = reduced.astype(jnp.bfloat16)
    held = lax.optimization_barrier(high_part)
    low_part = (reduced - held.astype(jnp.float32)).astype(jnp.bfloat16)
    return (high_part, low_part)


def parts_product(high_part, low_part, cotangent):
    dims = (((0,), (0,)), ((), ()))
    first_term = lax.dot_general(high_part, cotangent, dims, preferred_element_type=jnp.float32)
    second_term = lax.dot_general(low_part, cotangent, dims, preferred_element_type=jnp.float32)
    return first_term + second_term


def body(
    normed_input,
    query_cotangent,
    value_cotangent,
    query_basis,
    value_basis,
    query_weight,
    value_weight,
    query_first,
    query_second,
    value_first,
    value_second,
):
    row_count = query_weight.shape[0]
    query_width = query_cotangent.shape[1]
    offset = lax.axis_index(("fs", "rep")) * row_count
    query_rows = lax.dynamic_slice_in_dim(query_basis, offset, row_count, 0).astype(jnp.float32)
    value_rows = lax.dynamic_slice_in_dim(value_basis, offset, row_count, 0).astype(jnp.float32)
    reduced_query = jnp.dot(normed_input, query_basis, preferred_element_type=jnp.float32)
    reduced_value = jnp.dot(normed_input, value_basis, preferred_element_type=jnp.float32)
    query_high, query_low = split_parts(reduced_query)
    value_high, value_low = split_parts(reduced_value)
    projected = lax.psum_scatter(
        jnp.concatenate(
            [
                parts_product(query_high, query_low, query_cotangent),
                parts_product(value_high, value_low, value_cotangent),
            ],
            axis=1,
        ),
        ("fs", "rep"),
        scatter_dimension=0,
        tiled=True,
    )
    query_projected = projected[:, :query_width]
    value_projected = projected[:, query_width:]
    query_first_new, query_second_new, query_dir = moments(
        query_projected, query_first, query_second
    )
    value_first_new, value_second_new, value_dir = moments(
        value_projected, value_first, value_second
    )
    query_whole, value_whole = (
        lax.all_gather(query_dir, ("fs", "rep"), axis=0, tiled=True),
        lax.all_gather(value_dir, ("fs", "rep"), axis=0, tiled=True),
    )
    query_squares, value_squares = lax.psum(
        (jnp.sum(query_dir * query_dir), jnp.sum(value_dir * value_dir)), ("fs", "rep", "tp")
    )
    tp_count = lax.axis_size("tp")
    query_update, query_weight_new, query_half = finish(
        query_whole,
        query_rows,
        query_weight,
        query_squares,
        query_whole.shape[0] * query_whole.shape[1] * tp_count,
    )
    value_update, value_weight_new, value_half = finish(
        value_whole,
        value_rows,
        value_weight,
        value_squares,
        value_whole.shape[0] * value_whole.shape[1] * tp_count,
    )
    query_copy, value_copy = (
        lax.all_gather(query_half, ("fs", "rep"), axis=0, tiled=True),
        lax.all_gather(value_half, ("fs", "rep"), axis=0, tiled=True),
    )
    return (
        query_update,
        value_update,
        query_weight_new,
        value_weight_new,
        query_first_new,
        query_second_new,
        value_first_new,
        value_second_new,
        query_copy,
        value_copy,
    )


MESH = pl.DeviceIdType.MESH
VMEM_LIMIT = 60 * 2**20
OUT_LIMIT = 16 * 2**20
CHUNKS = (1, 0)
EARLY_Z = (2,)
PIECES = 2
FINAL = ('G0', 'G1', 'F0', 'F1', 'S0', 'S1', 'N1', '10', 'N0', '20', '11', '21', '30', '31')
OFF_Z = True
YIELD = 2
DIAG = ((0, 3),)
RELAY = {'third0': 1}
PLAN = {'second1': (('r', 0, 1, 1, None), ('r', 1, 1, 1, None), ('r', 0, 0, 1, None), ('r', 1, 0, 1, None)), 'recv12': (('z', 2, 1, 1, None),), 'recv10': (('r', 1, 1, 0, None), ('r', 0, 1, 0, None)), 'sent': (('z', 2, 0, 1, None), ('z', 2, 0, 0, None)), 'fourth0': (('z', 2, 1, 0, None),), 'third0': (('r', 0, 0, 0, None), ('r', 1, 0, 0, None))}
f32, bf16 = jnp.float32, jnp.bfloat16


def scope(name):
    pass


def two_parts(x):
    high = x.astype(bf16)
    return high, (x - high.astype(f32)).astype(bf16)


def size_of(ref):
    n = jnp.dtype(ref.dtype).itemsize
    for d in ref.shape:
        n *= d
    return n


def kernel(
    T,
    x_hbm, qc_hbm, vc_hbm, qb_hbm, vb_hbm, qw_hbm, vw_hbm, qf_hbm, qs_hbm, vf_hbm, vs_hbm,
    qu, vu, qn, vn, qfn, vfn, qsn, vsn, qcopy, vcopy,
    x_ref, qc, vc, qb, vb, qw, vw, qf, vf, qs, vs,
    qzw, vzw, qrw, vrw, qpart, vpart, qgot1, vgot1, qmid, vmid, qgot2, vgot2, qdirs, vdirs,
    norms, spare,
    load, sent, in1, in2, in3, in4, in5, in6, in7, in8, in9, in10, rest,
):
    F, R = 4, 4
    z, r, t = lax.axis_index("fs"), lax.axis_index("rep"), lax.axis_index("tp")
    zs = [z, z + 1 - 2 * lax.rem(z, 2), 3 - z, lax.rem(z + 2, 4)]
    rs = [r, r + 1 - 2 * lax.rem(r, 2), lax.rem(r + 2, 4), 3 - r]
    ts = [lax.rem(t + k, T) for k in range(T)]
    rows, M = qw.shape[0], qf.shape[0]
    cot, basis, weight, first, second = (qc, vc), (qb, vb), (qw, vw), (qf, vf), (qs, vs)
    update_out, weight_out, first_out, second_out = (qu, vu), (qn, vn), (qfn, vfn), (qsn, vsn)
    copy, z_weight, r_weight = (qcopy, vcopy), (qzw, vzw), (qrw, vrw)
    part, got1, mid, got2, dirs = (qpart, vpart), (qgot1, vgot1), (qmid, vmid), (qgot2, vgot2), (qdirs, vdirs)
    width = [w.shape[1] for w in weight]

    total_sent, total_rest = [], []

    def remote(src, dst, received, peer, last=False):
        d = pltpu.make_async_remote_copy(
            src_ref=src,
            dst_ref=dst,
            send_sem=sent.at[0],
            recv_sem=received,
            device_id=peer,
            device_id_type=MESH,
        )
        d.start()
        total_sent.append(size_of(src))
        if last:
            total_rest.append(size_of(src))
        return d

    def settle(ref, sem):
        pltpu.make_async_copy(ref, ref, sem).wait()

    scope("p00_sig_load")
    barrier = pltpu.get_barrier_semaphore()
    for axis, others in (("rep", rs), ("fs", zs), ("tp", ts)):
        for other in others[1:]:
            pl.semaphore_signal(barrier, inc=1, device_id={axis: other}, device_id_type=MESH)
    sources = {
        "x": (x_hbm, x_ref),
        ("basis", 0): (qb_hbm, qb), ("cot", 0): (qc_hbm, qc),
        ("basis", 1): (vb_hbm, vb), ("cot", 1): (vc_hbm, vc),
        ("weight", 0): (qw_hbm, qw), ("weight", 1): (vw_hbm, vw),
        ("first", 0): (qf_hbm, qf), ("first", 1): (vf_hbm, vf),
        ("second", 0): (qs_hbm, qs), ("second", 1): (vs_hbm, vs),
    }
    c0, c1 = CHUNKS
    groups = [
        ["x", ("basis", c0)],
        [("cot", c0)],
        [("basis", c1), ("cot", c1)],
        [("weight", c0), ("weight", c1)],
        [(n, c) for n in ("first", "second") for c in CHUNKS],
    ]
    for i, group in enumerate(groups):
        for n in group:
            pltpu.make_async_copy(*sources[n], load.at[i]).start()

    def loaded(i):
        settle(spare.at[: sum(size_of(sources[n][1]) for n in groups[i]) // 512], load.at[i])

    def run(point):
        if point in RELAY:
            c = CHUNKS[RELAY[point]]
            settle(z_weight[c].at[0], in8.at[c, 1])
            remote(z_weight[c].at[1], z_weight[c].at[2], in8.at[c, 2], {"fs": zs[1]})
        for core in (None, 0, 1):
            pieces = [q[:4] for q in PLAN.get(point, ()) if q[4] == core]
            if pieces:
                by_core(core, functools.partial(send_pieces, pieces))

    def send_pieces(pieces):
        for kind, k, c, p in pieces:
            part_rows = pl.ds(p * (rows // PIECES), rows // PIECES)
            source = weight[c].at[part_rows]
            if kind == "z":
                remote(source, z_weight[c].at[k - 1, part_rows], in8.at[c, k - 1], {"fs": zs[k]})
            else:
                remote(source, r_weight[c].at[k, part_rows], in9.at[c, k], {"rep": rs[k + 1]})

    def by_core(core, body):
        if core is None:
            return body()
        scope(None)
        n, m = len(total_sent), len(total_rest)
        pl.when(t == core)(body)
        if core > 0:
            del total_sent[n:]
            del total_rest[m:]

    far = (2, 3, 1, 0)

    def send_first(c):
        for j in far:
            for k in range(1, R):
                remote(part[c].at[rs[k], zs[j]], got1[c].at[k, j], in1.at[c, j], {"rep": rs[k]})

    for i, c in enumerate(CHUNKS):
        scope(f"p01_load_dot#c={c}")
        loaded(2 * i)
        if i == 0:
            x = x_ref[...]
        reduced = jnp.dot(x, basis[c][...], preferred_element_type=f32).T
        high, low = two_parts(reduced)
        both = jnp.concatenate([high, low], axis=1)
        if i == 0:
            loaded(1)
        g = cot[c][...]
        total = jnp.dot(both, jnp.concatenate([g, g], axis=0), preferred_element_type=f32)
        for a in range(F):
            for b in range(R):
                at = (a * R + b) * M
                part[c][b, a] = total[at : at + M]
        if i == 0:
            scope("p02_barrier")
            pl.semaphore_wait(barrier, F + R + T - 3)
        scope(f"p03_send1#c={c}")
        by_core(0 if i and YIELD else None, functools.partial(send_first, c))
    loaded(3)
    run("sent")

    own = {}
    for c in CHUNKS:
        scope(f"p04_recv1#c={c}")
        for n, j in enumerate(far):
            if YIELD and c == CHUNKS[0] and n == YIELD - 1:
                by_core(1, functools.partial(send_first, CHUNKS[1]))
            total = part[c][r, zs[j]]
            settle(got1[c].at[1:R, j], in1.at[c, j])
            for k in range(1, R):
                total = total + got1[c][k, j]
            if j > 0:
                mid[c][j] = total
                remote(mid[c].at[j], got2[c].at[j], in2.at[c], {"fs": zs[j]})
            else:
                own[c] = total
            run(f"recv{CHUNKS.index(c)}{n}")
        run(f"second{CHUNKS.index(c)}")

    third, sums = {}, []

    def spread(c, j):
        block = dirs[c].at[zs[j], r]
        for k in range(1, R):
            remote(block, block, in4.at[c], {"rep": rs[k]})

    for c in CHUNKS:
        scope(f"p05_recv2#c={c}")
        if c == c0:
            loaded(4)
        projected = own[c]
        settle(got2[c].at[1:F], in2.at[c])
        for j in (1, 3, 2):
            projected = projected + got2[c][j]
        fn = 0.9 * first[c][...] + 0.1 * projected
        sn = 0.99 * second[c][...] + 0.01 * projected * projected
        dirs[c][z, r] = fn / (jnp.sqrt(sn) + 1e-08)
        sums.append(jnp.sum(dirs[c][z, r] * dirs[c][z, r], keepdims=True))
        if c == CHUNKS[-1]:
            scope("p055_norms")
            lane = lax.broadcasted_iota(jnp.int32, (1, 128), 1)
            slot = (z * R + r) * T + t
            norms[slot] = jnp.where(lane < 64, sums[CHUNKS.index(0)], sums[CHUNKS.index(1)])
            for j in far:
                for k in range(R):
                    for n in range(T):
                        if j or k or n:
                            peer = {"fs": zs[j], "rep": rs[k], "tp": ts[n]}
                            remote(norms.at[slot], norms.at[slot], in5.at[0], peer)
            scope(f"p056_third#c={c}")
        block = dirs[c].at[z, r]
        for j in (2, 3, 1):
            third[c, j] = remote(block, block, in3.at[c, j - 1], {"fs": zs[j]})
        spread(c, 0)
        first_out[c][...] = fn
        second_out[c][...] = sn
        run(f"third{CHUNKS.index(c)}")

    for c in CHUNKS:
        scope(f"p06_recv3#c={c}")
        for n, j in enumerate((1, 3, 2)):
            third[c, j].wait_recv()
            spread(c, j)
            run(f"spread{CHUNKS.index(c)}{n}")
        run(f"fourth{CHUNKS.index(c)}")

    def start_of(j, k):
        return pl.multiple_of((zs[j] * R + rs[k]) * rows, rows)

    size = rows // 2

    def piece(c, j, k, p):
        at = pl.multiple_of(start_of(j, k) + p * size, size)
        return copy[c].at[pl.ds(at, size), :]

    def product(c, dd, blocks):
        b = jnp.concatenate([basis[c][pl.ds(start_of(j, k), rows), :] for j, k in blocks], axis=0)
        return jnp.dot(jnp.concatenate([b, b], axis=1), dd, preferred_element_type=f32)

    direct, across, sixth = {}, {}, {}

    def pass_on(c, j, a):
        block = piece(c, j, a + 1, a)
        remote(block, block, rest.at[0], {"rep": rs[2 - a]}, True)

    def send_direct(c, j, order=((0, 0), (1, 1), (0, 1), (1, 0))):
        if (CHUNKS.index(c), j) in DIAG:
            block = copy[c].at[pl.ds(start_of(j, 0), rows), :]
            for k in (3, 1, 2):
                remote(block, block, rest.at[0], {"rep": rs[k]}, True)
            return
        for a, p in order:
            block = piece(c, j, 0, p)
            if a == p:
                direct[c, j, a] = remote(block, block, in7.at[c, j - 2, a], {"rep": rs[a + 1]})
            else:
                remote(block, block, rest.at[0], {"rep": rs[a + 1]}, True)

    late = [j for j in range(1, F) if j not in EARLY_Z and not (OFF_Z and j == 1)]
    waiting, sq = [], None

    def gather(c):
        nonlocal sq
        scope(f"p07_recv4#c={c}")
        settle(dirs[c].at[:, 1:R], in4.at[c])
        scope(f"p08_square#c={c}")
        whole = dirs[c][...].reshape(F * R * M, width[c])
        dd = jnp.concatenate(two_parts(whole), axis=0)
        relayed = CHUNKS.index(c) in RELAY.values()
        blocks = [(0, 0), (0, 1), (0, 2), (2, 0)] + ([(3, 0)] if relayed else [])
        raw = product(c, dd, blocks[:3])
        raw_far = product(c, dd, blocks[3:]) if blocks[3:] else None
        scope(f"p09_fifth#c={c}")
        if c == CHUNKS[0]:
            settle(spare.at[: F * R * T - 1], in5.at[0])
            sq = jnp.sum(norms[...].reshape(F * R * T, 128), axis=0, keepdims=True)
        count = F * R * M * width[c] * T
        inverse = 1.0 / jnp.sqrt(sq[:, 64 * c : 64 * c + 1] / count + 1.0)
        scope(f"p10_copy#c={c}")
        for n, (j, k) in enumerate(blocks):
            source = raw if n < 3 else raw_far
            at = n if n < 3 else n - 3
            update = source[at * rows : (at + 1) * rows] * inverse
            if n == 0:
                new = weight[c][...] - 0.01 * update
                update_out[c][...] = update
                weight_out[c][...] = new
            elif k == 0:
                waiting.append((c, j, update))
                continue
            else:
                settle(r_weight[c].at[0], in9.at[c, k - 1])
                new = r_weight[c][k - 1] - 0.01 * update
            copy[c][pl.ds(start_of(j, k), rows), :] = new.astype(bf16)
            if k > 0 and OFF_Z:
                block = piece(c, 0, k, k - 1)
                across[c, k - 1] = remote(block, block, in10.at[c, k - 1], {"fs": zs[1]})
        for a in range(2):
            pass_on(c, 0, a)

    def others(c):
        for k in (1, 2):
            block = piece(c, 0, k, 2 - k)
            remote(block, block, rest.at[0], {"fs": zs[1]}, True)
        block = copy[c].at[pl.ds(start_of(0, 0), rows), :]
        remote(block, block, rest.at[0], {"fs": zs[1]}, True)

    def far_rows(c):
        for owner, j, update in waiting:
            if owner == c:
                scope(f"p115_far#c={c}")
                relayed = CHUNKS.index(c) in RELAY.values()
                if not relayed or j == 3:
                    settle(z_weight[c].at[0], in8.at[c, j - 1])
                new = z_weight[c][j - 1] - 0.01 * update
                copy[c][pl.ds(start_of(j, 0), rows), :] = new.astype(bf16)
                if not relayed:
                    block = copy[c].at[pl.ds(start_of(j, 0), rows), :]
                    sixth[c, 3] = remote(block, block, in6.at[c, 0], {"fs": zs[1]})
                send_direct(c, j)

    def sixth_rows(c):
        if CHUNKS.index(c) in RELAY.values():
            return
        scope(f"p12_sixth#c={c}")
        for j in late:
            sixth[c, j].wait_recv()
            send_direct(c, j)

    def pass_rows(c, j):
        if (CHUNKS.index(c), j) in DIAG:
            return
        scope(f"p13_pass#c={c}#j={j}")
        for a in range(2):
            (across[c, a] if OFF_Z and j == 1 else direct[c, j, a]).wait_recv()
            pass_on(c, j, a)

    for step in FINAL:
        c = CHUNKS[int(step[1])]
        if step[0] == "N":
            others(c)
        elif step[0] == "G":
            gather(c)
        elif step[0] in "OP":
            by_core(0 if step[0] == "O" else 1, functools.partial(others, c))
        elif step[0] == "F":
            far_rows(c)
        elif step[0] == "S":
            sixth_rows(c)
        else:
            pass_rows(c, int(step[0]))
    scope("p15_last")
    settle(spare.at[: sum(total_rest) // 512], rest.at[0])
    scope("p16_waitsend")
    settle(spare.at[: sum(total_sent) // 512], sent.at[0])
    scope(None)


def write_out(*refs):
    sem, sources, targets = refs[-1].at[0], refs[:10], refs[10:20]
    copies = [pltpu.make_async_copy(src, dst, sem) for src, dst in zip(sources, targets)]
    for c in copies[::-1]:
        c.start()
    whole = refs[-2].at[: sum(size_of(src) for src in sources) // 512]
    pltpu.make_async_copy(whole, whole, sem).wait()


def fused(plain, *args):
    x, qc, vc, qb, vb, qw, vw, qf, qs, vf, vs = args
    F, R, T = (lax.axis_size(name) for name in ("fs", "rep", "tp"))
    QC, VC = qc.shape[1], vc.shape[1]
    M, rows = qf.shape[0], qw.shape[0]
    aligned = M % 8 == 0 and rows % 32 == 0 and QC % 128 == 0 and VC % 128 == 0
    if not aligned or F != 4 or R != 4:
        return plain(*args)
    out = jax.ShapeDtypeStruct
    vmem = pl.BlockSpec(memory_space=pltpu.VMEM)
    dma = pltpu.SemaphoreType.DMA
    W = (QC, VC)

    def each(*shape, dtype=f32):
        return [pltpu.VMEM(shape + (w,), dtype) for w in W]

    sems = [
        (5,), (1,), (2, F), (2,), (2, F - 1), (2,), (1,), (2, 1), (2, 2, 2), (2, F - 1), (2, 2), (2, 2), (1,),
    ]
    results = pl.pallas_call(
        functools.partial(kernel, T),
        out_shape=each(rows) + each(rows) + each(M) + each(M) + each(rows * F * R, dtype=bf16),
        in_specs=[pl.BlockSpec(memory_space=pltpu.HBM)] * 11,
        out_specs=[vmem] * 10,
        scratch_shapes=[
            pltpu.VMEM(x.shape, bf16),
            pltpu.VMEM(qc.shape, bf16),
            pltpu.VMEM(vc.shape, bf16),
            pltpu.VMEM(qb.shape, bf16),
            pltpu.VMEM(vb.shape, bf16),
            *each(rows), *each(M), *each(M),
            *each(F - 1, rows), *each(2, rows),
            *each(R, F, M), *each(R, F, M), *each(F, M), *each(F, M), *each(F, R, M),
            pltpu.VMEM((F * R * T, 1, 128), f32),
            pltpu.VMEM((8 * rows * F * R, 128), f32),
            *[dma(shape) for shape in sems],
        ],
        compiler_params=pltpu.CompilerParams(
            collective_id=0, has_side_effects=True, vmem_limit_bytes=VMEM_LIMIT
        ),
    )(*args)
    outs = pl.pallas_call(
        write_out,
        out_shape=[
            out(qw.shape, f32), out(vw.shape, f32), out(qw.shape, f32), out(vw.shape, f32),
            out(qf.shape, f32), out(vf.shape, f32), out(qf.shape, f32), out(vf.shape, f32),
            out((rows * F * R, QC), bf16), out((rows * F * R, VC), bf16),
        ],
        in_specs=[vmem] * 10,
        out_specs=[pl.BlockSpec(memory_space=pltpu.HBM)] * 10,
        scratch_shapes=[pltpu.VMEM((8 * rows * F * R, 128), f32), dma((1,))],
        compiler_params=pltpu.CompilerParams(vmem_limit_bytes=OUT_LIMIT),
    )(*results)
    qu, vu, qn, vn, qfn, vfn, qsn, vsn, qcopy, vcopy = outs
    return (qu, vu, qn, vn, qfn, qsn, vfn, vsn, qcopy, vcopy)


def solution(mesh):
    in_specs = (
        P(("fs", "rep"), None),
        P(("fs", "rep"), "tp"),
        P(("fs", "rep"), "tp"),
        P(),
        P(),
        P(("fs", "rep"), "tp"),
        P(("fs", "rep"), "tp"),
        P(("fs", "rep"), "tp"),
        P(("fs", "rep"), "tp"),
        P(("fs", "rep"), "tp"),
        P(("fs", "rep"), "tp"),
    )
    out_specs = (
        P(("fs", "rep"), "tp"),
        P(("fs", "rep"), "tp"),
        P(("fs", "rep"), "tp"),
        P(("fs", "rep"), "tp"),
        P(("fs", "rep"), "tp"),
        P(("fs", "rep"), "tp"),
        P(("fs", "rep"), "tp"),
        P(("fs", "rep"), "tp"),
        P(None, "tp"),
        P(None, "tp"),
    )
    return jax.shard_map(functools.partial(fused, body), mesh=mesh, in_specs=in_specs, out_specs=out_specs, check_vma=False)
```

```python
import functools
import jax
import jax.numpy as jnp
from jax import lax
from jax.experimental import pallas as pl
from jax.experimental.pallas import tpu as pltpu
from jax.sharding import PartitionSpec as P


def moments(projected, first_old, second_old):
    first_new = 0.9 * first_old + 0.1 * projected
    second_new = 0.99 * second_old + 0.01 * projected * projected
    return (first_new, second_new, first_new / (jnp.sqrt(second_new) + 1e-08))


def finish(whole_dir, basis_rows, weight, squares, entries):
    norm_scale = jnp.sqrt(squares / entries + 1.0)
    update = jnp.dot(basis_rows, whole_dir, precision=lax.Precision.HIGHEST) / norm_scale
    weight_new = weight - 0.01 * update
    return (update, weight_new, weight_new.astype(jnp.bfloat16))


def split_parts(reduced):
    high_part = reduced.astype(jnp.bfloat16)
    held = lax.optimization_barrier(high_part)
    low_part = (reduced - held.astype(jnp.float32)).astype(jnp.bfloat16)
    return (high_part, low_part)


def parts_product(high_part, low_part, cotangent):
    dims = (((0,), (0,)), ((), ()))
    first_term = lax.dot_general(high_part, cotangent, dims, preferred_element_type=jnp.float32)
    second_term = lax.dot_general(low_part, cotangent, dims, preferred_element_type=jnp.float32)
    return first_term + second_term


def body(
    normed_input,
    query_cotangent,
    value_cotangent,
    query_basis,
    value_basis,
    query_weight,
    value_weight,
    query_first,
    query_second,
    value_first,
    value_second,
):
    row_count = query_weight.shape[0]
    query_width = query_cotangent.shape[1]
    offset = lax.axis_index(("fs", "rep")) * row_count
    query_rows = lax.dynamic_slice_in_dim(query_basis, offset, row_count, 0).astype(jnp.float32)
    value_rows = lax.dynamic_slice_in_dim(value_basis, offset, row_count, 0).astype(jnp.float32)
    reduced_query = jnp.dot(normed_input, query_basis, preferred_element_type=jnp.float32)
    reduced_value = jnp.dot(normed_input, value_basis, preferred_element_type=jnp.float32)
    query_high, query_low = split_parts(reduced_query)
    value_high, value_low = split_parts(reduced_value)
    projected = lax.psum_scatter(
        jnp.concatenate(
            [
                parts_product(query_high, query_low, query_cotangent),
                parts_product(value_high, value_low, value_cotangent),
            ],
            axis=1,
        ),
        ("fs", "rep"),
        scatter_dimension=0,
        tiled=True,
    )
    query_projected = projected[:, :query_width]
    value_projected = projected[:, query_width:]
    query_first_new, query_second_new, query_dir = moments(
        query_projected, query_first, query_second
    )
    value_first_new, value_second_new, value_dir = moments(
        value_projected, value_first, value_second
    )
    query_whole, value_whole = (
        lax.all_gather(query_dir, ("fs", "rep"), axis=0, tiled=True),
        lax.all_gather(value_dir, ("fs", "rep"), axis=0, tiled=True),
    )
    query_squares, value_squares = lax.psum(
        (jnp.sum(query_dir * query_dir), jnp.sum(value_dir * value_dir)), ("fs", "rep", "tp")
    )
    tp_count = lax.axis_size("tp")
    query_update, query_weight_new, query_half = finish(
        query_whole,
        query_rows,
        query_weight,
        query_squares,
        query_whole.shape[0] * query_whole.shape[1] * tp_count,
    )
    value_update, value_weight_new, value_half = finish(
        value_whole,
        value_rows,
        value_weight,
        value_squares,
        value_whole.shape[0] * value_whole.shape[1] * tp_count,
    )
    query_copy, value_copy = (
        lax.all_gather(query_half, ("fs", "rep"), axis=0, tiled=True),
        lax.all_gather(value_half, ("fs", "rep"), axis=0, tiled=True),
    )
    return (
        query_update,
        value_update,
        query_weight_new,
        value_weight_new,
        query_first_new,
        query_second_new,
        value_first_new,
        value_second_new,
        query_copy,
        value_copy,
    )


MESH = pl.DeviceIdType.MESH
VMEM_LIMIT = 60 * 2**20
OUT_LIMIT = 16 * 2**20
CHUNKS = (1, 0)
PIECES = 2
FINAL = ('G0', 'G1', 'F0', 'F1', 'O1', 'S1', 'O0', 'P1', 'S0', '10', '21', 'P0', '20', '11', '31', '30')
YIELD = 2
DIAG = ((0, 3), (1, 3))
RELAY = {'third1': 1}
PLAN = {'sent': (('z', 2, 0, 1, None), ('z', 2, 1, 1, 1), ('z', 2, 0, 0, None)), 'recv11': (('z', 2, 1, 1, 0), ('r', 0, 0, 0, None), ('r', 1, 0, 0, None)), 'second1': (('r', 0, 1, 1, None), ('r', 1, 1, 1, None), ('r', 1, 0, 1, None), ('r', 0, 0, 1, None)), 'recv10': (('r', 1, 1, 0, None), ('r', 0, 1, 0, None)), 'fourth0': (('z', 2, 1, 0, None),)}
f32, bf16 = jnp.float32, jnp.bfloat16


def two_parts(x):
    high = x.astype(bf16)
    return high, (x - high.astype(f32)).astype(bf16)


def size_of(ref):
    n = jnp.dtype(ref.dtype).itemsize
    for d in ref.shape:
        n *= d
    return n


def kernel(
    T,
    x_hbm, qc_hbm, vc_hbm, qb_hbm, vb_hbm, qw_hbm, vw_hbm, qf_hbm, qs_hbm, vf_hbm, vs_hbm,
    qu, vu, qn, vn, qfn, vfn, qsn, vsn, qcopy, vcopy,
    x_ref, qc, vc, qb, vb, qw, vw, qf, vf, qs, vs,
    qzw, vzw, qrw, vrw, qpart, vpart, qgot1, vgot1, qmid, vmid, qgot2, vgot2, qdirs, vdirs,
    norms, spare,
    load, sent, in1, in2, in3, in4, in5, in6, in7, in8, in9, in10, rest,
):
    F, R = 4, 4
    z, r, t = lax.axis_index("fs"), lax.axis_index("rep"), lax.axis_index("tp")
    zs = [z, z + 1 - 2 * lax.rem(z, 2), 3 - z, lax.rem(z + 2, 4)]
    rs = [r, r + 1 - 2 * lax.rem(r, 2), lax.rem(r + 2, 4), 3 - r]
    ts = [lax.rem(t + k, T) for k in range(T)]
    rows, M = qw.shape[0], qf.shape[0]
    cot, basis, weight, first, second = (qc, vc), (qb, vb), (qw, vw), (qf, vf), (qs, vs)
    update_out, weight_out, first_out, second_out = (qu, vu), (qn, vn), (qfn, vfn), (qsn, vsn)
    copy, z_weight, r_weight = (qcopy, vcopy), (qzw, vzw), (qrw, vrw)
    part, got1, mid, got2, dirs = (qpart, vpart), (qgot1, vgot1), (qmid, vmid), (qgot2, vgot2), (qdirs, vdirs)
    width = [w.shape[1] for w in weight]

    total_sent, total_rest = [], []

    def remote(src, dst, received, peer, last=False):
        d = pltpu.make_async_remote_copy(
            src_ref=src,
            dst_ref=dst,
            send_sem=sent.at[0],
            recv_sem=received,
            device_id=peer,
            device_id_type=MESH,
        )
        d.start()
        total_sent.append(size_of(src))
        if last:
            total_rest.append(size_of(src))
        return d

    def settle(ref, sem):
        pltpu.make_async_copy(ref, ref, sem).wait()

    barrier = pltpu.get_barrier_semaphore()
    for axis, others in (("rep", rs), ("fs", zs), ("tp", ts)):
        for other in others[1:]:
            pl.semaphore_signal(barrier, inc=1, device_id={axis: other}, device_id_type=MESH)
    sources = {
        "x": (x_hbm, x_ref),
        ("basis", 0): (qb_hbm, qb), ("cot", 0): (qc_hbm, qc),
        ("basis", 1): (vb_hbm, vb), ("cot", 1): (vc_hbm, vc),
        ("weight", 0): (qw_hbm, qw), ("weight", 1): (vw_hbm, vw),
        ("first", 0): (qf_hbm, qf), ("first", 1): (vf_hbm, vf),
        ("second", 0): (qs_hbm, qs), ("second", 1): (vs_hbm, vs),
    }
    c0, c1 = CHUNKS
    groups = [
        ["x", ("basis", c0)],
        [("cot", c0)],
        [("basis", c1), ("cot", c1)],
        [("weight", c0), ("weight", c1)],
        [(n, c) for n in ("first", "second") for c in CHUNKS],
    ]
    for i, group in enumerate(groups):
        for n in group:
            pltpu.make_async_copy(*sources[n], load.at[i]).start()

    def loaded(i):
        settle(spare.at[: sum(size_of(sources[n][1]) for n in groups[i]) // 512], load.at[i])

    def run(point):
        if point in RELAY:
            c = CHUNKS[RELAY[point]]
            settle(z_weight[c].at[0], in8.at[c, 0])
            remote(z_weight[c].at[1], z_weight[c].at[2], in8.at[c, 1], {"fs": zs[1]})
        for core in (None, 0, 1):
            pieces = [q[:4] for q in PLAN.get(point, ()) if q[4] == core]
            if pieces:
                by_core(core, functools.partial(send_pieces, pieces))

    def send_pieces(pieces):
        for kind, k, c, p in pieces:
            part_rows = pl.ds(p * (rows // PIECES), rows // PIECES)
            source = weight[c].at[part_rows]
            if kind == "z":
                remote(source, z_weight[c].at[k - 1, part_rows], in8.at[c, k - 2], {"fs": zs[k]})
            else:
                remote(source, r_weight[c].at[k, part_rows], in9.at[c], {"rep": rs[k + 1]})

    def by_core(core, body):
        if core is None:
            return body()
        n, m = len(total_sent), len(total_rest)
        pl.when(t == core)(body)
        if core > 0:
            del total_sent[n:]
            del total_rest[m:]

    far = (2, 3, 1, 0)

    def send_first(c):
        for j in far:
            for k in range(1, R):
                remote(part[c].at[rs[k], zs[j]], got1[c].at[k, j], in1.at[c, j], {"rep": rs[k]})

    for i, c in enumerate(CHUNKS):
        loaded(2 * i)
        if i == 0:
            x = x_ref[...]
        reduced = jnp.dot(x, basis[c][...], preferred_element_type=f32).T
        high, low = two_parts(reduced)
        both = jnp.concatenate([high, low], axis=1)
        if i == 0:
            loaded(1)
        g = cot[c][...]
        total = jnp.dot(both, jnp.concatenate([g, g], axis=0), preferred_element_type=f32)
        for a in range(F):
            for b in range(R):
                at = (a * R + b) * M
                part[c][b, a] = total[at : at + M]
        if i == 0:
            pl.semaphore_wait(barrier, F + R + T - 3)
        by_core(0 if i and YIELD else None, functools.partial(send_first, c))
    loaded(3)
    run("sent")

    own = {}
    for c in CHUNKS:
        for n, j in enumerate(far):
            if YIELD and c == CHUNKS[0] and n == YIELD - 1:
                by_core(1, functools.partial(send_first, CHUNKS[1]))
            total = part[c][r, zs[j]]
            settle(got1[c].at[1:R, j], in1.at[c, j])
            for k in range(1, R):
                total = total + got1[c][k, j]
            if j > 0:
                mid[c][j] = total
                remote(mid[c].at[j], got2[c].at[j], in2.at[c], {"fs": zs[j]})
            else:
                own[c] = total
            run(f"recv{CHUNKS.index(c)}{n}")
        run(f"second{CHUNKS.index(c)}")

    third, sums = {}, []

    def spread(c, j):
        block = dirs[c].at[zs[j], r]
        for k in range(1, R):
            remote(block, block, in4.at[c], {"rep": rs[k]})

    for c in CHUNKS:
        if c == c0:
            loaded(4)
        projected = own[c]
        settle(got2[c].at[1:F], in2.at[c])
        for j in (1, 3, 2):
            projected = projected + got2[c][j]
        fn = 0.9 * first[c][...] + 0.1 * projected
        sn = 0.99 * second[c][...] + 0.01 * projected * projected
        dirs[c][z, r] = fn / (jnp.sqrt(sn) + 1e-08)
        sums.append(jnp.sum(dirs[c][z, r] * dirs[c][z, r], keepdims=True))
        if c == CHUNKS[-1]:
            lane = lax.broadcasted_iota(jnp.int32, (1, 128), 1)
            slot = (z * R + r) * T + t
            norms[slot] = jnp.where(lane < 64, sums[CHUNKS.index(0)], sums[CHUNKS.index(1)])
            for j in far:
                for k in range(R):
                    for n in range(T):
                        if j or k or n:
                            peer = {"fs": zs[j], "rep": rs[k], "tp": ts[n]}
                            remote(norms.at[slot], norms.at[slot], in5.at[0], peer)
        block = dirs[c].at[z, r]
        for j in (2, 3, 1):
            third[c, j] = remote(block, block, in3.at[c, j - 1], {"fs": zs[j]})
        spread(c, 0)
        first_out[c][...] = fn
        second_out[c][...] = sn
        run(f"third{CHUNKS.index(c)}")

    for c in CHUNKS:
        for n, j in enumerate((1, 3, 2)):
            third[c, j].wait_recv()
            spread(c, j)
            run(f"spread{CHUNKS.index(c)}{n}")
        run(f"fourth{CHUNKS.index(c)}")

    def start_of(j, k):
        return pl.multiple_of((zs[j] * R + rs[k]) * rows, rows)

    size = rows // 2

    def piece(c, j, k, p):
        at = pl.multiple_of(start_of(j, k) + p * size, size)
        return copy[c].at[pl.ds(at, size), :]

    def product(c, dd, blocks):
        b = jnp.concatenate([basis[c][pl.ds(start_of(j, k), rows), :] for j, k in blocks], axis=0)
        return jnp.dot(jnp.concatenate([b, b], axis=1), dd, preferred_element_type=f32)

    direct, across, sixth = {}, {}, {}

    def pass_on(c, j, a):
        block = piece(c, j, a + 1, a)
        remote(block, block, rest.at[0], {"rep": rs[2 - a]}, True)

    def send_direct(c, j, order=((0, 0), (1, 1), (0, 1), (1, 0))):
        if (CHUNKS.index(c), j) in DIAG:
            block = copy[c].at[pl.ds(start_of(j, 0), rows), :]
            for k in (3, 1, 2):
                remote(block, block, rest.at[0], {"rep": rs[k]}, True)
            return
        for a, p in order:
            block = piece(c, j, 0, p)
            if a == p:
                direct[c, j, a] = remote(block, block, in7.at[c, j - 2, a], {"rep": rs[a + 1]})
            else:
                remote(block, block, rest.at[0], {"rep": rs[a + 1]}, True)

    waiting, sq = [], None

    def gather(c):
        nonlocal sq
        settle(dirs[c].at[:, 1:R], in4.at[c])
        whole = dirs[c][...].reshape(F * R * M, width[c])
        dd = jnp.concatenate(two_parts(whole), axis=0)
        relayed = CHUNKS.index(c) in RELAY.values()
        blocks = [(0, 0), (0, 1), (0, 2), (2, 0)] + ([(3, 0)] if relayed else [])
        raw = product(c, dd, blocks[:3])
        raw_far = product(c, dd, blocks[3:]) if blocks[3:] else None
        if c == CHUNKS[0]:
            settle(spare.at[: F * R * T - 1], in5.at[0])
            sq = jnp.sum(norms[...].reshape(F * R * T, 128), axis=0, keepdims=True)
        count = F * R * M * width[c] * T
        inverse = 1.0 / jnp.sqrt(sq[:, 64 * c : 64 * c + 1] / count + 1.0)
        for n, (j, k) in enumerate(blocks):
            source = raw if n < 3 else raw_far
            at = n if n < 3 else n - 3
            update = source[at * rows : (at + 1) * rows] * inverse
            if n == 0:
                new = weight[c][...] - 0.01 * update
                update_out[c][...] = update
                weight_out[c][...] = new
            elif k == 0:
                waiting.append((c, j, update))
                continue
            else:
                if k == 1:
                    settle(r_weight[c], in9.at[c])
                new = r_weight[c][k - 1] - 0.01 * update
            copy[c][pl.ds(start_of(j, k), rows), :] = new.astype(bf16)
            if k > 0:
                block = piece(c, 0, k, k - 1)
                across[c, k - 1] = remote(block, block, in10.at[c, k - 1], {"fs": zs[1]})
        for a in range(2):
            pass_on(c, 0, a)

    def others(c):
        for k in (1, 2):
            block = piece(c, 0, k, 2 - k)
            remote(block, block, rest.at[0], {"fs": zs[1]}, True)
        block = copy[c].at[pl.ds(start_of(0, 0), rows), :]
        remote(block, block, rest.at[0], {"fs": zs[1]}, True)

    def far_rows(c):
        for owner, j, update in waiting:
            if owner == c:
                relayed = CHUNKS.index(c) in RELAY.values()
                if not relayed or j == 3:
                    settle(z_weight[c].at[0], in8.at[c, j - 2])
                new = z_weight[c][j - 1] - 0.01 * update
                copy[c][pl.ds(start_of(j, 0), rows), :] = new.astype(bf16)
                if not relayed:
                    block = copy[c].at[pl.ds(start_of(j, 0), rows), :]
                    sixth[c, 3] = remote(block, block, in6.at[c, 0], {"fs": zs[1]})
                send_direct(c, j)

    def sixth_rows(c):
        if CHUNKS.index(c) in RELAY.values():
            return
        sixth[c, 3].wait_recv()
        send_direct(c, 3)

    def pass_rows(c, j):
        if (CHUNKS.index(c), j) in DIAG:
            return
        for a in range(2):
            (across[c, a] if j == 1 else direct[c, j, a]).wait_recv()
            pass_on(c, j, a)

    for step in FINAL:
        c = CHUNKS[int(step[1])]
        if step[0] == "N":
            others(c)
        elif step[0] == "G":
            gather(c)
        elif step[0] in "OP":
            by_core(0 if step[0] == "O" else 1, functools.partial(others, c))
        elif step[0] == "F":
            far_rows(c)
        elif step[0] == "S":
            sixth_rows(c)
        else:
            pass_rows(c, int(step[0]))
    settle(spare.at[: sum(total_rest) // 512], rest.at[0])
    settle(spare.at[: sum(total_sent) // 512], sent.at[0])


def write_out(*refs):
    sem, sources, targets = refs[-1].at[0], refs[:10], refs[10:20]
    copies = [pltpu.make_async_copy(src, dst, sem) for src, dst in zip(sources, targets)]
    for c in copies[::-1]:
        c.start()
    whole = refs[-2].at[: sum(size_of(src) for src in sources) // 512]
    pltpu.make_async_copy(whole, whole, sem).wait()


def fused(plain, *args):
    x, qc, vc, qb, vb, qw, vw, qf, qs, vf, vs = args
    F, R, T = (lax.axis_size(name) for name in ("fs", "rep", "tp"))
    QC, VC = qc.shape[1], vc.shape[1]
    M, rows = qf.shape[0], qw.shape[0]
    aligned = M % 8 == 0 and rows % 32 == 0 and QC % 128 == 0 and VC % 128 == 0
    if not aligned or F != 4 or R != 4:
        return plain(*args)
    out = jax.ShapeDtypeStruct
    vmem = pl.BlockSpec(memory_space=pltpu.VMEM)
    dma = pltpu.SemaphoreType.DMA
    W = (QC, VC)

    def each(*shape, dtype=f32):
        return [pltpu.VMEM(shape + (w,), dtype) for w in W]

    sems = [
        (5,), (1,), (2, F), (2,), (2, F - 1), (2,), (1,), (2, 1), (2, 2, 2), (2, 2), (2,), (2, 2), (1,),
    ]
    results = pl.pallas_call(
        functools.partial(kernel, T),
        out_shape=each(rows) + each(rows) + each(M) + each(M) + each(rows * F * R, dtype=bf16),
        in_specs=[pl.BlockSpec(memory_space=pltpu.HBM)] * 11,
        out_specs=[vmem] * 10,
        scratch_shapes=[
            pltpu.VMEM(x.shape, bf16),
            pltpu.VMEM(qc.shape, bf16),
            pltpu.VMEM(vc.shape, bf16),
            pltpu.VMEM(qb.shape, bf16),
            pltpu.VMEM(vb.shape, bf16),
            *each(rows), *each(M), *each(M),
            *each(F - 1, rows), *each(2, rows),
            *each(R, F, M), *each(R, F, M), *each(F, M), *each(F, M), *each(F, R, M),
            pltpu.VMEM((F * R * T, 1, 128), f32),
            pltpu.VMEM((8 * rows * F * R, 128), f32),
            *[dma(shape) for shape in sems],
        ],
        compiler_params=pltpu.CompilerParams(
            collective_id=0, has_side_effects=True, vmem_limit_bytes=VMEM_LIMIT
        ),
    )(*args)
    outs = pl.pallas_call(
        write_out,
        out_shape=[
            out(qw.shape, f32), out(vw.shape, f32), out(qw.shape, f32), out(vw.shape, f32),
            out(qf.shape, f32), out(vf.shape, f32), out(qf.shape, f32), out(vf.shape, f32),
            out((rows * F * R, QC), bf16), out((rows * F * R, VC), bf16),
        ],
        in_specs=[vmem] * 10,
        out_specs=[pl.BlockSpec(memory_space=pltpu.HBM)] * 10,
        scratch_shapes=[pltpu.VMEM((8 * rows * F * R, 128), f32), dma((1,))],
        compiler_params=pltpu.CompilerParams(vmem_limit_bytes=OUT_LIMIT),
    )(*results)
    qu, vu, qn, vn, qfn, vfn, qsn, vsn, qcopy, vcopy = outs
    return (qu, vu, qn, vn, qfn, qsn, vfn, vsn, qcopy, vcopy)


def solution(mesh):
    in_specs = (
        P(("fs", "rep"), None),
        P(("fs", "rep"), "tp"),
        P(("fs", "rep"), "tp"),
        P(),
        P(),
        P(("fs", "rep"), "tp"),
        P(("fs", "rep"), "tp"),
        P(("fs", "rep"), "tp"),
        P(("fs", "rep"), "tp"),
        P(("fs", "rep"), "tp"),
        P(("fs", "rep"), "tp"),
    )
    out_specs = (
        P(("fs", "rep"), "tp"),
        P(("fs", "rep"), "tp"),
        P(("fs", "rep"), "tp"),
        P(("fs", "rep"), "tp"),
        P(("fs", "rep"), "tp"),
        P(("fs", "rep"), "tp"),
        P(("fs", "rep"), "tp"),
        P(("fs", "rep"), "tp"),
        P(None, "tp"),
        P(None, "tp"),
    )
    return jax.shard_map(functools.partial(fused, body), mesh=mesh, in_specs=in_specs, out_specs=out_specs, check_vma=False)
```

```python
import functools
import jax
import jax.numpy as jnp
from jax import lax
from jax.experimental import pallas as pl
from jax.experimental.pallas import tpu as pltpu
from jax.sharding import PartitionSpec as P


def moments(projected, first_old, second_old):
    first_new = 0.9 * first_old + 0.1 * projected
    second_new = 0.99 * second_old + 0.01 * projected * projected
    return (first_new, second_new, first_new / (jnp.sqrt(second_new) + 1e-08))


def finish(whole_dir, basis_rows, weight, squares, entries):
    norm_scale = jnp.sqrt(squares / entries + 1.0)
    update = jnp.dot(basis_rows, whole_dir, precision=lax.Precision.HIGHEST) / norm_scale
    weight_new = weight - 0.01 * update
    return (update, weight_new, weight_new.astype(jnp.bfloat16))


def split_parts(reduced):
    high_part = reduced.astype(jnp.bfloat16)
    held = lax.optimization_barrier(high_part)
    low_part = (reduced - held.astype(jnp.float32)).astype(jnp.bfloat16)
    return (high_part, low_part)


def parts_product(high_part, low_part, cotangent):
    dims = (((0,), (0,)), ((), ()))
    first_term = lax.dot_general(high_part, cotangent, dims, preferred_element_type=jnp.float32)
    second_term = lax.dot_general(low_part, cotangent, dims, preferred_element_type=jnp.float32)
    return first_term + second_term


def body(
    normed_input,
    query_cotangent,
    value_cotangent,
    query_basis,
    value_basis,
    query_weight,
    value_weight,
    query_first,
    query_second,
    value_first,
    value_second,
):
    row_count = query_weight.shape[0]
    query_width = query_cotangent.shape[1]
    offset = lax.axis_index(("fs", "rep")) * row_count
    query_rows = lax.dynamic_slice_in_dim(query_basis, offset, row_count, 0).astype(jnp.float32)
    value_rows = lax.dynamic_slice_in_dim(value_basis, offset, row_count, 0).astype(jnp.float32)
    reduced_query = jnp.dot(normed_input, query_basis, preferred_element_type=jnp.float32)
    reduced_value = jnp.dot(normed_input, value_basis, preferred_element_type=jnp.float32)
    query_high, query_low = split_parts(reduced_query)
    value_high, value_low = split_parts(reduced_value)
    projected = lax.psum_scatter(
        jnp.concatenate(
            [
                parts_product(query_high, query_low, query_cotangent),
                parts_product(value_high, value_low, value_cotangent),
            ],
            axis=1,
        ),
        ("fs", "rep"),
        scatter_dimension=0,
        tiled=True,
    )
    query_projected = projected[:, :query_width]
    value_projected = projected[:, query_width:]
    query_first_new, query_second_new, query_dir = moments(
        query_projected, query_first, query_second
    )
    value_first_new, value_second_new, value_dir = moments(
        value_projected, value_first, value_second
    )
    query_whole, value_whole = (
        lax.all_gather(query_dir, ("fs", "rep"), axis=0, tiled=True),
        lax.all_gather(value_dir, ("fs", "rep"), axis=0, tiled=True),
    )
    query_squares, value_squares = lax.psum(
        (jnp.sum(query_dir * query_dir), jnp.sum(value_dir * value_dir)), ("fs", "rep", "tp")
    )
    tp_count = lax.axis_size("tp")
    query_update, query_weight_new, query_half = finish(
        query_whole,
        query_rows,
        query_weight,
        query_squares,
        query_whole.shape[0] * query_whole.shape[1] * tp_count,
    )
    value_update, value_weight_new, value_half = finish(
        value_whole,
        value_rows,
        value_weight,
        value_squares,
        value_whole.shape[0] * value_whole.shape[1] * tp_count,
    )
    query_copy, value_copy = (
        lax.all_gather(query_half, ("fs", "rep"), axis=0, tiled=True),
        lax.all_gather(value_half, ("fs", "rep"), axis=0, tiled=True),
    )
    return (
        query_update,
        value_update,
        query_weight_new,
        value_weight_new,
        query_first_new,
        query_second_new,
        value_first_new,
        value_second_new,
        query_copy,
        value_copy,
    )


MESH = pl.DeviceIdType.MESH
VMEM_LIMIT = 60 * 2**20
OUT_LIMIT = 16 * 2**20
CHUNKS = (1, 0)
PIECES = 2
FINAL = ('G0', 'G1', 'F0', 'F1', 'O1', 'S1', 'O0', 'P1', 'S0', '10', '21', 'P0', '20', '11', '31', '30')
YIELD = 2
DIAG = ((0, 3), (1, 3))
RELAY = {'third1': 1}
PLAN = {'sent': (('z', 2, 0, 1, None), ('z', 2, 1, 1, 1), ('z', 2, 0, 0, None)), 'recv11': (('z', 2, 1, 1, 0), ('r', 0, 0, 0, None), ('r', 1, 0, 0, None)), 'second1': (('r', 0, 1, 1, None), ('r', 1, 1, 1, None), ('r', 1, 0, 1, None), ('r', 0, 0, 1, None)), 'recv10': (('r', 1, 1, 0, None), ('r', 0, 1, 0, None)), 'fourth0': (('z', 2, 1, 0, None),)}
f32, bf16 = jnp.float32, jnp.bfloat16


def two_parts(x):
    high = x.astype(bf16)
    return high, (x - high.astype(f32)).astype(bf16)


def size_of(ref):
    n = jnp.dtype(ref.dtype).itemsize
    for d in ref.shape:
        n *= d
    return n


def kernel(
    T,
    x_hbm, qc_hbm, vc_hbm, qb_hbm, vb_hbm, qw_hbm, vw_hbm, qf_hbm, qs_hbm, vf_hbm, vs_hbm,
    qu, vu, qn, vn, qfn, vfn, qsn, vsn, qcopy, vcopy,
    x_ref, qc, vc, qb, vb, qw, vw, qf, vf, qs, vs,
    qzw, vzw, qrw, vrw, qpart, vpart, qgot1, vgot1, qmid, vmid, qgot2, vgot2, qdirs, vdirs,
    norms, spare,
    load, sent, in1, in2, in3, in4, in5, in6, in7, in8, in9, in10, rest,
):
    F, R = 4, 4
    z, r, t = lax.axis_index("fs"), lax.axis_index("rep"), lax.axis_index("tp")
    zs = [z, z + 1 - 2 * lax.rem(z, 2), 3 - z, lax.rem(z + 2, 4)]
    rs = [r, r + 1 - 2 * lax.rem(r, 2), lax.rem(r + 2, 4), 3 - r]
    ts = [lax.rem(t + k, T) for k in range(T)]
    rows, M = qw.shape[0], qf.shape[0]
    cot, basis, weight, first, second = (qc, vc), (qb, vb), (qw, vw), (qf, vf), (qs, vs)
    update_out, weight_out, first_out, second_out = (qu, vu), (qn, vn), (qfn, vfn), (qsn, vsn)
    copy, z_weight, r_weight = (qcopy, vcopy), (qzw, vzw), (qrw, vrw)
    part, got1, mid, got2, dirs = (qpart, vpart), (qgot1, vgot1), (qmid, vmid), (qgot2, vgot2), (qdirs, vdirs)
    width = [w.shape[1] for w in weight]

    total_sent, total_rest = [], []

    def remote(src, dst, received, peer, last=False):
        d = pltpu.make_async_remote_copy(
            src_ref=src,
            dst_ref=dst,
            send_sem=sent.at[0],
            recv_sem=received,
            device_id=peer,
            device_id_type=MESH,
        )
        d.start()
        total_sent.append(size_of(src))
        if last:
            total_rest.append(size_of(src))
        return d

    def settle(ref, sem):
        pltpu.make_async_copy(ref, ref, sem).wait()

    barrier = pltpu.get_barrier_semaphore()
    for axis, others in (("rep", rs), ("fs", zs), ("tp", ts)):
        for other in others[1:]:
            pl.semaphore_signal(barrier, inc=1, device_id={axis: other}, device_id_type=MESH)
    sources = {
        "x": (x_hbm, x_ref),
        ("basis", 0): (qb_hbm, qb), ("cot", 0): (qc_hbm, qc),
        ("basis", 1): (vb_hbm, vb), ("cot", 1): (vc_hbm, vc),
        ("weight", 0): (qw_hbm, qw), ("weight", 1): (vw_hbm, vw),
        ("first", 0): (qf_hbm, qf), ("first", 1): (vf_hbm, vf),
        ("second", 0): (qs_hbm, qs), ("second", 1): (vs_hbm, vs),
    }
    c0, c1 = CHUNKS
    groups = [
        ["x", ("basis", c0)],
        [("cot", c0)],
        [("basis", c1), ("cot", c1)],
        [("weight", c0), ("weight", c1)],
        [(n, c) for n in ("first", "second") for c in CHUNKS],
    ]
    for i, group in enumerate(groups):
        for n in group:
            pltpu.make_async_copy(*sources[n], load.at[i]).start()

    def loaded(i):
        settle(spare.at[: sum(size_of(sources[n][1]) for n in groups[i]) // 512], load.at[i])

    def run(point):
        if point in RELAY:
            c = CHUNKS[RELAY[point]]
            settle(z_weight[c].at[0], in8.at[c, 0])
            remote(z_weight[c].at[1], z_weight[c].at[2], in8.at[c, 1], {"fs": zs[1]})
        for core in (None, 0, 1):
            pieces = [q[:4] for q in PLAN.get(point, ()) if q[4] == core]
            if pieces:
                by_core(core, functools.partial(send_pieces, pieces))

    def send_pieces(pieces):
        for kind, k, c, p in pieces:
            part_rows = pl.ds(p * (rows // PIECES), rows // PIECES)
            source = weight[c].at[part_rows]
            if kind == "z":
                remote(source, z_weight[c].at[k - 1, part_rows], in8.at[c, k - 2], {"fs": zs[k]})
            else:
                remote(source, r_weight[c].at[k, part_rows], in9.at[c], {"rep": rs[k + 1]})

    def by_core(core, body):
        if core is None:
            return body()
        n, m = len(total_sent), len(total_rest)
        pl.when(t == core)(body)
        if core > 0:
            del total_sent[n:]
            del total_rest[m:]

    far = (2, 3, 1, 0)

    def send_first(c):
        for j in far:
            for k in range(1, R):
                remote(part[c].at[rs[k], zs[j]], got1[c].at[k, j], in1.at[c, j], {"rep": rs[k]})

    for i, c in enumerate(CHUNKS):
        loaded(2 * i)
        if i == 0:
            x = x_ref[...]
        reduced = jnp.dot(x, basis[c][...], preferred_element_type=f32).T
        high, low = two_parts(reduced)
        both = jnp.concatenate([high, low], axis=1)
        if i == 0:
            loaded(1)
        g = cot[c][...]
        total = jnp.dot(both, jnp.concatenate([g, g], axis=0), preferred_element_type=f32)
        for a in range(F):
            for b in range(R):
                at = (a * R + b) * M
                part[c][b, a] = total[at : at + M]
        if i == 0:
            pl.semaphore_wait(barrier, F + R + T - 3)
        by_core(0 if i and YIELD else None, functools.partial(send_first, c))
    loaded(3)
    run("sent")

    own = {}
    for c in CHUNKS:
        for n, j in enumerate(far):
            if YIELD and c == CHUNKS[0] and n == YIELD - 1:
                by_core(1, functools.partial(send_first, CHUNKS[1]))
            total = part[c][r, zs[j]]
            settle(got1[c].at[1:R, j], in1.at[c, j])
            for k in range(1, R):
                total = total + got1[c][k, j]
            if j > 0:
                mid[c][j] = total
                remote(mid[c].at[j], got2[c].at[j], in2.at[c], {"fs": zs[j]})
            else:
                own[c] = total
            run(f"recv{CHUNKS.index(c)}{n}")
        run(f"second{CHUNKS.index(c)}")

    third, sums = {}, []

    def spread(c, j):
        block = dirs[c].at[zs[j], r]
        for k in range(1, R):
            remote(block, block, in4.at[c], {"rep": rs[k]})

    for c in CHUNKS:
        if c == c0:
            loaded(4)
        projected = own[c]
        settle(got2[c].at[1:F], in2.at[c])
        for j in (1, 3, 2):
            projected = projected + got2[c][j]
        fn = 0.9 * first[c][...] + 0.1 * projected
        sn = 0.99 * second[c][...] + 0.01 * projected * projected
        dirs[c][z, r] = fn / (jnp.sqrt(sn) + 1e-08)
        sums.append(jnp.sum(dirs[c][z, r] * dirs[c][z, r], keepdims=True))
        block = dirs[c].at[z, r]
        for j in (2, 3, 1):
            third[c, j] = remote(block, block, in3.at[c, j - 1], {"fs": zs[j]})
        spread(c, 0)
        if c == CHUNKS[-1]:
            lane = lax.broadcasted_iota(jnp.int32, (1, 128), 1)
            slot = (z * R + r) * T + t
            norms[slot] = jnp.where(lane < 64, sums[CHUNKS.index(0)], sums[CHUNKS.index(1)])
            for j in far:
                for k in range(R):
                    for n in range(T):
                        if j or k or n:
                            peer = {"fs": zs[j], "rep": rs[k], "tp": ts[n]}
                            remote(norms.at[slot], norms.at[slot], in5.at[0], peer)
        first_out[c][...] = fn
        second_out[c][...] = sn
        run(f"third{CHUNKS.index(c)}")

    for c in CHUNKS:
        for n, j in enumerate((1, 3, 2)):
            third[c, j].wait_recv()
            spread(c, j)
            run(f"spread{CHUNKS.index(c)}{n}")
        run(f"fourth{CHUNKS.index(c)}")

    def start_of(j, k):
        return pl.multiple_of((zs[j] * R + rs[k]) * rows, rows)

    size = rows // 2

    def piece(c, j, k, p):
        at = pl.multiple_of(start_of(j, k) + p * size, size)
        return copy[c].at[pl.ds(at, size), :]

    def product(c, dd, blocks):
        b = jnp.concatenate([basis[c][pl.ds(start_of(j, k), rows), :] for j, k in blocks], axis=0)
        return jnp.dot(jnp.concatenate([b, b], axis=1), dd, preferred_element_type=f32)

    direct, across, sixth = {}, {}, {}

    def pass_on(c, j, a):
        block = piece(c, j, a + 1, a)
        remote(block, block, rest.at[0], {"rep": rs[2 - a]}, True)

    def send_direct(c, j, order=((0, 0), (1, 1), (0, 1), (1, 0))):
        if (CHUNKS.index(c), j) in DIAG:
            block = copy[c].at[pl.ds(start_of(j, 0), rows), :]
            for k in (3, 1, 2):
                remote(block, block, rest.at[0], {"rep": rs[k]}, True)
            return
        for a, p in order:
            block = piece(c, j, 0, p)
            if a == p:
                direct[c, j, a] = remote(block, block, in7.at[c, j - 2, a], {"rep": rs[a + 1]})
            else:
                remote(block, block, rest.at[0], {"rep": rs[a + 1]}, True)

    waiting, sq = [], None

    def gather(c):
        nonlocal sq
        settle(dirs[c].at[:, 1:R], in4.at[c])
        whole = dirs[c][...].reshape(F * R * M, width[c])
        dd = jnp.concatenate(two_parts(whole), axis=0)
        relayed = CHUNKS.index(c) in RELAY.values()
        blocks = [(0, 0), (0, 1), (0, 2), (2, 0)] + ([(3, 0)] if relayed else [])
        raw = product(c, dd, blocks[:3])
        raw_far = product(c, dd, blocks[3:]) if blocks[3:] else None
        if c == CHUNKS[0]:
            settle(spare.at[: F * R * T - 1], in5.at[0])
            sq = jnp.sum(norms[...].reshape(F * R * T, 128), axis=0, keepdims=True)
        count = F * R * M * width[c] * T
        inverse = 1.0 / jnp.sqrt(sq[:, 64 * c : 64 * c + 1] / count + 1.0)
        for n, (j, k) in enumerate(blocks):
            source = raw if n < 3 else raw_far
            at = n if n < 3 else n - 3
            update = source[at * rows : (at + 1) * rows] * inverse
            if n == 0:
                new = weight[c][...] - 0.01 * update
                update_out[c][...] = update
                weight_out[c][...] = new
            elif k == 0:
                waiting.append((c, j, update))
                continue
            else:
                if k == 1:
                    settle(r_weight[c], in9.at[c])
                new = r_weight[c][k - 1] - 0.01 * update
            copy[c][pl.ds(start_of(j, k), rows), :] = new.astype(bf16)
            if k > 0:
                block = piece(c, 0, k, k - 1)
                across[c, k - 1] = remote(block, block, in10.at[c, k - 1], {"fs": zs[1]})
        for a in range(2):
            pass_on(c, 0, a)

    def others(c):
        for k in (1, 2):
            block = piece(c, 0, k, 2 - k)
            remote(block, block, rest.at[0], {"fs": zs[1]}, True)
        block = copy[c].at[pl.ds(start_of(0, 0), rows), :]
        remote(block, block, rest.at[0], {"fs": zs[1]}, True)

    def far_rows(c):
        for owner, j, update in waiting:
            if owner == c:
                relayed = CHUNKS.index(c) in RELAY.values()
                if not relayed or j == 3:
                    settle(z_weight[c].at[0], in8.at[c, j - 2])
                new = z_weight[c][j - 1] - 0.01 * update
                copy[c][pl.ds(start_of(j, 0), rows), :] = new.astype(bf16)
                if not relayed:
                    block = copy[c].at[pl.ds(start_of(j, 0), rows), :]
                    sixth[c, 3] = remote(block, block, in6.at[c, 0], {"fs": zs[1]})
                send_direct(c, j)

    def sixth_rows(c):
        if CHUNKS.index(c) in RELAY.values():
            return
        sixth[c, 3].wait_recv()
        send_direct(c, 3)

    def pass_rows(c, j):
        if (CHUNKS.index(c), j) in DIAG:
            return
        for a in range(2):
            (across[c, a] if j == 1 else direct[c, j, a]).wait_recv()
            pass_on(c, j, a)

    for step in FINAL:
        c = CHUNKS[int(step[1])]
        if step[0] == "N":
            others(c)
        elif step[0] == "G":
            gather(c)
        elif step[0] in "OP":
            by_core(0 if step[0] == "O" else 1, functools.partial(others, c))
        elif step[0] == "F":
            far_rows(c)
        elif step[0] == "S":
            sixth_rows(c)
        else:
            pass_rows(c, int(step[0]))
    settle(spare.at[: sum(total_rest) // 512], rest.at[0])
    settle(spare.at[: sum(total_sent) // 512], sent.at[0])


def write_out(*refs):
    sem, sources, targets = refs[-1].at[0], refs[:10], refs[10:20]
    copies = [pltpu.make_async_copy(src, dst, sem) for src, dst in zip(sources, targets)]
    for c in copies[::-1]:
        c.start()
    whole = refs[-2].at[: sum(size_of(src) for src in sources) // 512]
    pltpu.make_async_copy(whole, whole, sem).wait()


def fused(plain, *args):
    x, qc, vc, qb, vb, qw, vw, qf, qs, vf, vs = args
    F, R, T = (lax.axis_size(name) for name in ("fs", "rep", "tp"))
    QC, VC = qc.shape[1], vc.shape[1]
    M, rows = qf.shape[0], qw.shape[0]
    aligned = M % 8 == 0 and rows % 32 == 0 and QC % 128 == 0 and VC % 128 == 0
    if not aligned or F != 4 or R != 4:
        return plain(*args)
    out = jax.ShapeDtypeStruct
    vmem = pl.BlockSpec(memory_space=pltpu.VMEM)
    dma = pltpu.SemaphoreType.DMA
    W = (QC, VC)

    def each(*shape, dtype=f32):
        return [pltpu.VMEM(shape + (w,), dtype) for w in W]

    sems = [
        (5,), (1,), (2, F), (2,), (2, F - 1), (2,), (1,), (2, 1), (2, 2, 2), (2, 2), (2,), (2, 2), (1,),
    ]
    results = pl.pallas_call(
        functools.partial(kernel, T),
        out_shape=each(rows) + each(rows) + each(M) + each(M) + each(rows * F * R, dtype=bf16),
        in_specs=[pl.BlockSpec(memory_space=pltpu.HBM)] * 11,
        out_specs=[vmem] * 10,
        scratch_shapes=[
            pltpu.VMEM(x.shape, bf16),
            pltpu.VMEM(qc.shape, bf16),
            pltpu.VMEM(vc.shape, bf16),
            pltpu.VMEM(qb.shape, bf16),
            pltpu.VMEM(vb.shape, bf16),
            *each(rows), *each(M), *each(M),
            *each(F - 1, rows), *each(2, rows),
            *each(R, F, M), *each(R, F, M), *each(F, M), *each(F, M), *each(F, R, M),
            pltpu.VMEM((F * R * T, 1, 128), f32),
            pltpu.VMEM((8 * rows * F * R, 128), f32),
            *[dma(shape) for shape in sems],
        ],
        compiler_params=pltpu.CompilerParams(
            collective_id=0, has_side_effects=True, vmem_limit_bytes=VMEM_LIMIT
        ),
    )(*args)
    outs = pl.pallas_call(
        write_out,
        out_shape=[
            out(qw.shape, f32), out(vw.shape, f32), out(qw.shape, f32), out(vw.shape, f32),
            out(qf.shape, f32), out(vf.shape, f32), out(qf.shape, f32), out(vf.shape, f32),
            out((rows * F * R, QC), bf16), out((rows * F * R, VC), bf16),
        ],
        in_specs=[vmem] * 10,
        out_specs=[pl.BlockSpec(memory_space=pltpu.HBM)] * 10,
        scratch_shapes=[pltpu.VMEM((8 * rows * F * R, 128), f32), dma((1,))],
        compiler_params=pltpu.CompilerParams(vmem_limit_bytes=OUT_LIMIT),
    )(*results)
    qu, vu, qn, vn, qfn, vfn, qsn, vsn, qcopy, vcopy = outs
    return (qu, vu, qn, vn, qfn, qsn, vfn, vsn, qcopy, vcopy)


def solution(mesh):
    in_specs = (
        P(("fs", "rep"), None),
        P(("fs", "rep"), "tp"),
        P(("fs", "rep"), "tp"),
        P(),
        P(),
        P(("fs", "rep"), "tp"),
        P(("fs", "rep"), "tp"),
        P(("fs", "rep"), "tp"),
        P(("fs", "rep"), "tp"),
        P(("fs", "rep"), "tp"),
        P(("fs", "rep"), "tp"),
    )
    out_specs = (
        P(("fs", "rep"), "tp"),
        P(("fs", "rep"), "tp"),
        P(("fs", "rep"), "tp"),
        P(("fs", "rep"), "tp"),
        P(("fs", "rep"), "tp"),
        P(("fs", "rep"), "tp"),
        P(("fs", "rep"), "tp"),
        P(("fs", "rep"), "tp"),
        P(None, "tp"),
        P(None, "tp"),
    )
    return jax.shard_map(functools.partial(fused, body), mesh=mesh, in_specs=in_specs, out_specs=out_specs, check_vma=False)
```

```python
import functools
import jax
import jax.numpy as jnp
from jax import lax
from jax.experimental import pallas as pl
from jax.experimental.pallas import tpu as pltpu
from jax.sharding import PartitionSpec as P


def moments(projected, first_old, second_old):
    first_new = 0.9 * first_old + 0.1 * projected
    second_new = 0.99 * second_old + 0.01 * projected * projected
    return (first_new, second_new, first_new / (jnp.sqrt(second_new) + 1e-08))


def finish(whole_dir, basis_rows, weight, squares, entries):
    norm_scale = jnp.sqrt(squares / entries + 1.0)
    update = jnp.dot(basis_rows, whole_dir, precision=lax.Precision.HIGHEST) / norm_scale
    weight_new = weight - 0.01 * update
    return (update, weight_new, weight_new.astype(jnp.bfloat16))


def split_parts(reduced):
    high_part = reduced.astype(jnp.bfloat16)
    held = lax.optimization_barrier(high_part)
    low_part = (reduced - held.astype(jnp.float32)).astype(jnp.bfloat16)
    return (high_part, low_part)


def parts_product(high_part, low_part, cotangent):
    dims = (((0,), (0,)), ((), ()))
    first_term = lax.dot_general(high_part, cotangent, dims, preferred_element_type=jnp.float32)
    second_term = lax.dot_general(low_part, cotangent, dims, preferred_element_type=jnp.float32)
    return first_term + second_term


def body(
    normed_input,
    query_cotangent,
    value_cotangent,
    query_basis,
    value_basis,
    query_weight,
    value_weight,
    query_first,
    query_second,
    value_first,
    value_second,
):
    row_count = query_weight.shape[0]
    query_width = query_cotangent.shape[1]
    offset = lax.axis_index(("fs", "rep")) * row_count
    query_rows = lax.dynamic_slice_in_dim(query_basis, offset, row_count, 0).astype(jnp.float32)
    value_rows = lax.dynamic_slice_in_dim(value_basis, offset, row_count, 0).astype(jnp.float32)
    reduced_query = jnp.dot(normed_input, query_basis, preferred_element_type=jnp.float32)
    reduced_value = jnp.dot(normed_input, value_basis, preferred_element_type=jnp.float32)
    query_high, query_low = split_parts(reduced_query)
    value_high, value_low = split_parts(reduced_value)
    projected = lax.psum_scatter(
        jnp.concatenate(
            [
                parts_product(query_high, query_low, query_cotangent),
                parts_product(value_high, value_low, value_cotangent),
            ],
            axis=1,
        ),
        ("fs", "rep"),
        scatter_dimension=0,
        tiled=True,
    )
    query_projected = projected[:, :query_width]
    value_projected = projected[:, query_width:]
    query_first_new, query_second_new, query_dir = moments(
        query_projected, query_first, query_second
    )
    value_first_new, value_second_new, value_dir = moments(
        value_projected, value_first, value_second
    )
    query_whole, value_whole = (
        lax.all_gather(query_dir, ("fs", "rep"), axis=0, tiled=True),
        lax.all_gather(value_dir, ("fs", "rep"), axis=0, tiled=True),
    )
    query_squares, value_squares = lax.psum(
        (jnp.sum(query_dir * query_dir), jnp.sum(value_dir * value_dir)), ("fs", "rep", "tp")
    )
    tp_count = lax.axis_size("tp")
    query_update, query_weight_new, query_half = finish(
        query_whole,
        query_rows,
        query_weight,
        query_squares,
        query_whole.shape[0] * query_whole.shape[1] * tp_count,
    )
    value_update, value_weight_new, value_half = finish(
        value_whole,
        value_rows,
        value_weight,
        value_squares,
        value_whole.shape[0] * value_whole.shape[1] * tp_count,
    )
    query_copy, value_copy = (
        lax.all_gather(query_half, ("fs", "rep"), axis=0, tiled=True),
        lax.all_gather(value_half, ("fs", "rep"), axis=0, tiled=True),
    )
    return (
        query_update,
        value_update,
        query_weight_new,
        value_weight_new,
        query_first_new,
        query_second_new,
        value_first_new,
        value_second_new,
        query_copy,
        value_copy,
    )


MESH = pl.DeviceIdType.MESH
VMEM_LIMIT = 60 * 2**20
OUT_LIMIT = 16 * 2**20
CHUNKS = (1, 0)
PIECES = 2
FINAL = ('G0', 'G1', 'F0', 'F1', 'O1', 'S1', 'O0', 'P1', 'S0', '10', '21', 'P0', '20', '11', '31', '30')
YIELD = 2
DIAG = ((0, 3), (1, 3))
RELAY = {'third1': 1}
PLAN = {'sent': (('z', 2, 0, 1, None), ('z', 2, 1, 1, 1), ('z', 2, 0, 0, None)), 'recv11': (('z', 2, 1, 1, 0), ('r', 0, 0, 0, None), ('r', 1, 0, 0, None)), 'second1': (('r', 0, 1, 1, None), ('r', 1, 1, 1, None), ('r', 1, 0, 1, None), ('r', 0, 0, 1, None)), 'recv10': (('r', 1, 1, 0, None), ('r', 0, 1, 0, None)), 'fourth0': (('z', 2, 1, 0, None),)}
f32, bf16 = jnp.float32, jnp.bfloat16


def two_parts(x):
    high = x.astype(bf16)
    return high, (x - high.astype(f32)).astype(bf16)


def size_of(ref):
    n = jnp.dtype(ref.dtype).itemsize
    for d in ref.shape:
        n *= d
    return n


def kernel(
    T,
    x_hbm, qc_hbm, vc_hbm, qb_hbm, vb_hbm, qw_hbm, vw_hbm, qf_hbm, qs_hbm, vf_hbm, vs_hbm,
    qu, vu, qn, vn, qfn, vfn, qsn, vsn, qcopy, vcopy,
    x_ref, qc, vc, qb, vb, qw, vw, qf, vf, qs, vs,
    qzw, vzw, qrw, vrw, qpart, vpart, qgot1, vgot1, qmid, vmid, qgot2, vgot2, qdirs, vdirs,
    norms, spare,
    load, sent, in1, in2, in3, in4, in5, in6, in7, in8, in9, in10, rest,
):
    F, R = 4, 4
    z, r, t = lax.axis_index("fs"), lax.axis_index("rep"), lax.axis_index("tp")
    zs = [z, z + 1 - 2 * lax.rem(z, 2), 3 - z, lax.rem(z + 2, 4)]
    rs = [r, r + 1 - 2 * lax.rem(r, 2), lax.rem(r + 2, 4), 3 - r]
    ts = [lax.rem(t + k, T) for k in range(T)]
    rows, M = qw.shape[0], qf.shape[0]
    cot, basis, weight, first, second = (qc, vc), (qb, vb), (qw, vw), (qf, vf), (qs, vs)
    update_out, weight_out, first_out, second_out = (qu, vu), (qn, vn), (qfn, vfn), (qsn, vsn)
    copy, z_weight, r_weight = (qcopy, vcopy), (qzw, vzw), (qrw, vrw)
    part, got1, mid, got2, dirs = (qpart, vpart), (qgot1, vgot1), (qmid, vmid), (qgot2, vgot2), (qdirs, vdirs)
    width = [w.shape[1] for w in weight]

    total_sent, total_rest = [], []

    def remote(src, dst, received, peer, last=False):
        d = pltpu.make_async_remote_copy(
            src_ref=src,
            dst_ref=dst,
            send_sem=sent.at[0],
            recv_sem=received,
            device_id=peer,
            device_id_type=MESH,
        )
        d.start()
        total_sent.append(size_of(src))
        if last:
            total_rest.append(size_of(src))
        return d

    def settle(ref, sem):
        pltpu.make_async_copy(ref, ref, sem).wait()

    barrier = pltpu.get_barrier_semaphore()
    for axis, others in (("rep", rs), ("fs", zs), ("tp", ts)):
        for other in others[1:]:
            pl.semaphore_signal(barrier, inc=1, device_id={axis: other}, device_id_type=MESH)
    sources = {
        "x": (x_hbm, x_ref),
        ("basis", 0): (qb_hbm, qb), ("cot", 0): (qc_hbm, qc),
        ("basis", 1): (vb_hbm, vb), ("cot", 1): (vc_hbm, vc),
        ("weight", 0): (qw_hbm, qw), ("weight", 1): (vw_hbm, vw),
        ("first", 0): (qf_hbm, qf), ("first", 1): (vf_hbm, vf),
        ("second", 0): (qs_hbm, qs), ("second", 1): (vs_hbm, vs),
    }
    c0, c1 = CHUNKS
    groups = [
        ["x", ("basis", c0)],
        [("cot", c0)],
        [("basis", c1), ("cot", c1)],
        [("weight", c0), ("weight", c1)],
        [(n, c) for n in ("first", "second") for c in CHUNKS],
    ]
    for i, group in enumerate(groups):
        for n in group:
            pltpu.make_async_copy(*sources[n], load.at[i]).start()

    def loaded(i):
        settle(spare.at[: sum(size_of(sources[n][1]) for n in groups[i]) // 512], load.at[i])

    def run(point):
        if point in RELAY:
            c = CHUNKS[RELAY[point]]
            settle(z_weight[c].at[0], in8.at[c, 0])
            remote(z_weight[c].at[1], z_weight[c].at[2], in8.at[c, 1], {"fs": zs[1]})
        for core in (None, 0, 1):
            pieces = [q[:4] for q in PLAN.get(point, ()) if q[4] == core]
            if pieces:
                by_core(core, functools.partial(send_pieces, pieces))

    def send_pieces(pieces):
        for kind, k, c, p in pieces:
            part_rows = pl.ds(p * (rows // PIECES), rows // PIECES)
            source = weight[c].at[part_rows]
            if kind == "z":
                remote(source, z_weight[c].at[k - 1, part_rows], in8.at[c, k - 2], {"fs": zs[k]})
            else:
                remote(source, r_weight[c].at[k, part_rows], in9.at[c], {"rep": rs[k + 1]})

    def by_core(core, body):
        if core is None:
            return body()
        n, m = len(total_sent), len(total_rest)
        pl.when(t == core)(body)
        if core > 0:
            del total_sent[n:]
            del total_rest[m:]

    far = (2, 3, 1, 0)

    def send_first(c):
        for j in far:
            for k in range(1, R):
                remote(part[c].at[rs[k], zs[j]], got1[c].at[k, j], in1.at[c, j], {"rep": rs[k]})

    for i, c in enumerate(CHUNKS):
        loaded(2 * i)
        if i == 0:
            x = x_ref[...]
        reduced = jnp.dot(x, basis[c][...], preferred_element_type=f32).T
        high, low = two_parts(reduced)
        both = jnp.concatenate([high, low], axis=1)
        if i == 0:
            loaded(1)
        g = cot[c][...]
        total = jnp.dot(both, jnp.concatenate([g, g], axis=0), preferred_element_type=f32)
        for a in range(F):
            for b in range(R):
                at = (a * R + b) * M
                part[c][b, a] = total[at : at + M]
        if i == 0:
            pl.semaphore_wait(barrier, F + R + T - 3)
        by_core(0 if i and YIELD else None, functools.partial(send_first, c))
    loaded(3)
    run("sent")

    own = {}
    for c in CHUNKS:
        for n, j in enumerate(far):
            if YIELD and c == CHUNKS[0] and n == YIELD - 1:
                by_core(1, functools.partial(send_first, CHUNKS[1]))
            total = part[c][r, zs[j]]
            settle(got1[c].at[1:R, j], in1.at[c, j])
            for k in range(1, R):
                total = total + got1[c][k, j]
            if j > 0:
                mid[c][j] = total
                remote(mid[c].at[j], got2[c].at[j], in2.at[c], {"fs": zs[j]})
            else:
                own[c] = total
            run(f"recv{CHUNKS.index(c)}{n}")
        run(f"second{CHUNKS.index(c)}")

    third, sums = {}, []

    def spread(c, j):
        block = dirs[c].at[zs[j], r]
        for k in range(1, R):
            remote(block, block, in4.at[c], {"rep": rs[k]})

    for c in CHUNKS:
        if c == c0:
            loaded(4)
        projected = own[c]
        settle(got2[c].at[1:F], in2.at[c])
        for j in (1, 3, 2):
            projected = projected + got2[c][j]
        fn = 0.9 * first[c][...] + 0.1 * projected
        sn = 0.99 * second[c][...] + 0.01 * projected * projected
        dirs[c][z, r] = fn / (jnp.sqrt(sn) + 1e-08)
        sums.append(jnp.sum(dirs[c][z, r] * dirs[c][z, r], keepdims=True))
        block = dirs[c].at[z, r]
        for j in (2, 3, 1):
            third[c, j] = remote(block, block, in3.at[c, j - 1], {"fs": zs[j]})
        spread(c, 0)
        if c == CHUNKS[-1]:
            lane = lax.broadcasted_iota(jnp.int32, (1, 128), 1)
            slot = (z * R + r) * T + t
            norms[slot] = jnp.where(lane < 64, sums[CHUNKS.index(0)], sums[CHUNKS.index(1)])
            for j in far:
                for k in range(R):
                    for n in range(T):
                        if j or k or n:
                            peer = {"fs": zs[j], "rep": rs[k], "tp": ts[n]}
                            remote(norms.at[slot], norms.at[slot], in5.at[0], peer)
        first_out[c][...] = fn
        second_out[c][...] = sn
        run(f"third{CHUNKS.index(c)}")

    for c in CHUNKS:
        for n, j in enumerate((1, 3, 2)):
            third[c, j].wait_recv()
            spread(c, j)
            run(f"spread{CHUNKS.index(c)}{n}")
        run(f"fourth{CHUNKS.index(c)}")

    def start_of(j, k):
        return pl.multiple_of((zs[j] * R + rs[k]) * rows, rows)

    size = rows // 2

    def piece(c, j, k, p):
        at = pl.multiple_of(start_of(j, k) + p * size, size)
        return copy[c].at[pl.ds(at, size), :]

    def product(c, dd, blocks):
        b = jnp.concatenate([basis[c][pl.ds(start_of(j, k), rows), :] for j, k in blocks], axis=0)
        return jnp.dot(jnp.concatenate([b, b], axis=1), dd, preferred_element_type=f32)

    direct, across, sixth = {}, {}, {}

    def pass_on(c, j, a):
        block = piece(c, j, a + 1, a)
        remote(block, block, rest.at[0], {"rep": rs[2 - a]}, True)

    def send_direct(c, j, order=((0, 0), (1, 1), (0, 1), (1, 0))):
        if (CHUNKS.index(c), j) in DIAG:
            block = copy[c].at[pl.ds(start_of(j, 0), rows), :]
            for k in (3, 1, 2):
                remote(block, block, rest.at[0], {"rep": rs[k]}, True)
            return
        for a, p in order:
            block = piece(c, j, 0, p)
            if a == p:
                direct[c, j, a] = remote(block, block, in7.at[c, a], {"rep": rs[a + 1]})
            else:
                remote(block, block, rest.at[0], {"rep": rs[a + 1]}, True)

    waiting, sq = [], None

    def gather(c):
        nonlocal sq
        settle(dirs[c].at[:, 1:R], in4.at[c])
        whole = dirs[c][...].reshape(F * R * M, width[c])
        dd = jnp.concatenate(two_parts(whole), axis=0)
        relayed = CHUNKS.index(c) in RELAY.values()
        blocks = [(0, 0), (0, 1), (0, 2), (2, 0)] + ([(3, 0)] if relayed else [])
        raw = product(c, dd, blocks[:3])
        raw_far = product(c, dd, blocks[3:]) if blocks[3:] else None
        if c == CHUNKS[0]:
            settle(spare.at[: F * R * T - 1], in5.at[0])
            sq = jnp.sum(norms[...].reshape(F * R * T, 128), axis=0, keepdims=True)
        count = F * R * M * width[c] * T
        inverse = 1.0 / jnp.sqrt(sq[:, 64 * c : 64 * c + 1] / count + 1.0)
        for n, (j, k) in enumerate(blocks):
            source = raw if n < 3 else raw_far
            at = n if n < 3 else n - 3
            update = source[at * rows : (at + 1) * rows] * inverse
            if n == 0:
                new = weight[c][...] - 0.01 * update
                update_out[c][...] = update
                weight_out[c][...] = new
            elif k == 0:
                waiting.append((c, j, update))
                continue
            else:
                if k == 1:
                    settle(r_weight[c], in9.at[c])
                new = r_weight[c][k - 1] - 0.01 * update
            copy[c][pl.ds(start_of(j, k), rows), :] = new.astype(bf16)
            if k > 0:
                block = piece(c, 0, k, k - 1)
                across[c, k - 1] = remote(block, block, in10.at[c, k - 1], {"fs": zs[1]})
        for a in range(2):
            pass_on(c, 0, a)

    def others(c):
        for k in (1, 2):
            block = piece(c, 0, k, 2 - k)
            remote(block, block, rest.at[0], {"fs": zs[1]}, True)
        block = copy[c].at[pl.ds(start_of(0, 0), rows), :]
        remote(block, block, rest.at[0], {"fs": zs[1]}, True)

    def far_rows(c):
        for owner, j, update in waiting:
            if owner == c:
                relayed = CHUNKS.index(c) in RELAY.values()
                if not relayed or j == 3:
                    settle(z_weight[c].at[0], in8.at[c, j - 2])
                new = z_weight[c][j - 1] - 0.01 * update
                copy[c][pl.ds(start_of(j, 0), rows), :] = new.astype(bf16)
                if not relayed:
                    block = copy[c].at[pl.ds(start_of(j, 0), rows), :]
                    sixth[c, 3] = remote(block, block, in6.at[0], {"fs": zs[1]})
                send_direct(c, j)

    def sixth_rows(c):
        if CHUNKS.index(c) in RELAY.values():
            return
        sixth[c, 3].wait_recv()
        send_direct(c, 3)

    def pass_rows(c, j):
        if (CHUNKS.index(c), j) in DIAG:
            return
        for a in range(2):
            (across[c, a] if j == 1 else direct[c, j, a]).wait_recv()
            pass_on(c, j, a)

    for step in FINAL:
        c = CHUNKS[int(step[1])]
        if step[0] == "N":
            others(c)
        elif step[0] == "G":
            gather(c)
        elif step[0] in "OP":
            by_core(0 if step[0] == "O" else 1, functools.partial(others, c))
        elif step[0] == "F":
            far_rows(c)
        elif step[0] == "S":
            sixth_rows(c)
        else:
            pass_rows(c, int(step[0]))
    settle(spare.at[: sum(total_rest) // 512], rest.at[0])
    settle(spare.at[: sum(total_sent) // 512], sent.at[0])


def write_out(*refs):
    sem, sources, targets = refs[-1].at[0], refs[:10], refs[10:20]
    copies = [pltpu.make_async_copy(src, dst, sem) for src, dst in zip(sources, targets)]
    for c in copies[::-1]:
        c.start()
    whole = refs[-2].at[: sum(size_of(src) for src in sources) // 512]
    pltpu.make_async_copy(whole, whole, sem).wait()


def fused(plain, *args):
    x, qc, vc, qb, vb, qw, vw, qf, qs, vf, vs = args
    F, R, T = (lax.axis_size(name) for name in ("fs", "rep", "tp"))
    QC, VC = qc.shape[1], vc.shape[1]
    M, rows = qf.shape[0], qw.shape[0]
    aligned = M % 8 == 0 and rows % 32 == 0 and QC % 128 == 0 and VC % 128 == 0
    if not aligned or F != 4 or R != 4:
        return plain(*args)
    out = jax.ShapeDtypeStruct
    vmem = pl.BlockSpec(memory_space=pltpu.VMEM)
    dma = pltpu.SemaphoreType.DMA
    W = (QC, VC)

    def each(*shape, dtype=f32):
        return [pltpu.VMEM(shape + (w,), dtype) for w in W]

    sems = [
        (5,), (1,), (2, F), (2,), (2, F - 1), (2,), (1,), (1,), (2, 2), (2, 2), (2,), (2, 2), (1,),
    ]
    results = pl.pallas_call(
        functools.partial(kernel, T),
        out_shape=each(rows) + each(rows) + each(M) + each(M) + each(rows * F * R, dtype=bf16),
        in_specs=[pl.BlockSpec(memory_space=pltpu.HBM)] * 11,
        out_specs=[vmem] * 10,
        scratch_shapes=[
            pltpu.VMEM(x.shape, bf16),
            pltpu.VMEM(qc.shape, bf16),
            pltpu.VMEM(vc.shape, bf16),
            pltpu.VMEM(qb.shape, bf16),
            pltpu.VMEM(vb.shape, bf16),
            *each(rows), *each(M), *each(M),
            *each(F - 1, rows), *each(2, rows),
            *each(R, F, M), *each(R, F, M), *each(F, M), *each(F, M), *each(F, R, M),
            pltpu.VMEM((F * R * T, 1, 128), f32),
            pltpu.VMEM((8 * rows * F * R, 128), f32),
            *[dma(shape) for shape in sems],
        ],
        compiler_params=pltpu.CompilerParams(
            collective_id=0, has_side_effects=True, vmem_limit_bytes=VMEM_LIMIT
        ),
    )(*args)
    outs = pl.pallas_call(
        write_out,
        out_shape=[
            out(qw.shape, f32), out(vw.shape, f32), out(qw.shape, f32), out(vw.shape, f32),
            out(qf.shape, f32), out(vf.shape, f32), out(qf.shape, f32), out(vf.shape, f32),
            out((rows * F * R, QC), bf16), out((rows * F * R, VC), bf16),
        ],
        in_specs=[vmem] * 10,
        out_specs=[pl.BlockSpec(memory_space=pltpu.HBM)] * 10,
        scratch_shapes=[pltpu.VMEM((8 * rows * F * R, 128), f32), dma((1,))],
        compiler_params=pltpu.CompilerParams(vmem_limit_bytes=OUT_LIMIT),
    )(*results)
    qu, vu, qn, vn, qfn, vfn, qsn, vsn, qcopy, vcopy = outs
    return (qu, vu, qn, vn, qfn, qsn, vfn, vsn, qcopy, vcopy)


def solution(mesh):
    in_specs = (
        P(("fs", "rep"), None),
        P(("fs", "rep"), "tp"),
        P(("fs", "rep"), "tp"),
        P(),
        P(),
        P(("fs", "rep"), "tp"),
        P(("fs", "rep"), "tp"),
        P(("fs", "rep"), "tp"),
        P(("fs", "rep"), "tp"),
        P(("fs", "rep"), "tp"),
        P(("fs", "rep"), "tp"),
    )
    out_specs = (
        P(("fs", "rep"), "tp"),
        P(("fs", "rep"), "tp"),
        P(("fs", "rep"), "tp"),
        P(("fs", "rep"), "tp"),
        P(("fs", "rep"), "tp"),
        P(("fs", "rep"), "tp"),
        P(("fs", "rep"), "tp"),
        P(("fs", "rep"), "tp"),
        P(None, "tp"),
        P(None, "tp"),
    )
    return jax.shard_map(functools.partial(fused, body), mesh=mesh, in_specs=in_specs, out_specs=out_specs, check_vma=False)
```
